512 devices in a mesh: sp: 32 (over z, x), tp: 16 (over y, core).
Axes of the slice: x: 4, y: 8, z: 8, core: 2. Of those that a mesh axis runs over, the one named last changes fastest.
Arguments:
- cotangent: bfloat16 [4096, 2048], P('sp'), may hold values from -6 to 6
- mixer_out: bfloat16 [4096, 2048], P('sp'), may hold values from -6 to 6
- expert_ids: int32 [4096, 2], P('sp'), may hold values from 0 to 31, all different within a row; in each aligned block of 128 rows (0 to 127, 128 to 255, ...) at most 16 rows name the same one
- route_weight: float32 [4096, 2], P('sp'), may hold values from 0.3 to 1.5
- saved_normalized: bfloat16 [4096, 2048], P('sp', 'tp'), may hold values from -6 to 6
- inverse_deviation: float32 [4096], P('sp'), may hold values from 0.3 to 3
- channel_norm_gain: float32 [2048], P('tp'), may hold values from 0.1 to 1.9
- taps: float32 [31, 2048], P(None, 'tp'), may hold values from -1 to 1
- proj_weight: bfloat16 [2048, 2048], P('tp'), may hold values from -0.125 to 0.125
- gate_weight: bfloat16 [32, 2048, 2048], P('sp', None, 'tp'), may hold values from -0.125 to 0.125
- up_weight: bfloat16 [32, 2048, 2048], P('sp', None, 'tp'), may hold values from -0.125 to 0.125
- down_weight: bfloat16 [32, 2048, 2048], P('sp', 'tp'), may hold values from -0.125 to 0.125
Outputs:
- grad_mixer_in: bfloat16 [4096, 2048], P('sp', 'tp')
- grad_proj: float32 [2048, 2048], P('sp', 'tp')
- grad_gate: bfloat16 [32, 2048, 2048], P('sp', None, 'tp')
- grad_up: bfloat16 [32, 2048, 2048], P('sp', None, 'tp')
- grad_down: bfloat16 [32, 2048, 2048], P('sp', 'tp')
The draws below stay inside these ranges and needn't reach their ends.
Inputs may be any that keep to these rules, and one draw needn't show every extreme that they name: `expert_ids`: each row names 2 different experts. Within the rows of one index of sp no expert is named more than 16 times, a bound that some block reaches.
All inputs are finite; a program needn't handle non-finite values.
Results may differ from the reference program's by a relative error of at most 0.02.
Values may be sent and summed in bfloat16 or wider, within the bound.
No kernel may reach another device: no remote copies, remote signals or barrier semaphores. Data moves between devices by JAX's collectives and lax.ppermute only.
A program may use at most 64 MiB of HBM per device.

```python
import math
import jax
import jax.numpy as jnp
import numpy as np
from jax import lax

D = 2048
CHANNELS = 2048
EXPERT_FF = 2048
WIDTH = 31
TOPK = 2
TOK_DEV = 128
TOKENS = 4096
EXPERTS = 32
CAP = 16
FFD = 128
N_SP = 32
N_TP = 16


def spiked(drawn, own_key, source, target, blocks, factor):
    def block_of(dim):
        return (jnp.arange(drawn.shape[dim]) // (drawn.shape[dim] // blocks)).reshape((-1,) + (1,) * (drawn.ndim - 1 - dim))

    near = jax.random.permutation(own_key, blocks)[block_of(target)]
    second = (block_of(target) + blocks // 2) % blocks
    return jnp.where((block_of(source) == near) | (block_of(source) == second), factor * drawn, drawn)


def block_scale(rng, extent, split, smallest, high):
    def one(axis_at, blocks):
        draws = jax.random.uniform(jax.random.fold_in(jax.random.fold_in(rng, 6), axis_at), (blocks,), jnp.float32, smallest / len(split), high / len(split))
        return jnp.repeat(jnp.exp(draws), extent[axis_at] // blocks).reshape((-1,) + (1,) * (len(extent) - axis_at - 1))

    loudness = one(*split[0])
    for cut in split[1:]:
        loudness = loudness * one(*cut)
    return loudness


def deal_out(stream_key, own, number, rows, amount, top, reach, skew):
    sequence = jax.random.permutation(stream_key, amount)
    crowded, usual = portions_of(amount, rows * top, reach, skew, True), portions_of(amount, rows * top, reach, skew, False)
    places = jnp.arange(amount)

    def named(lengths, offset_by):
        used = int((lengths > 0).sum())
        fixed = max(1, used // 4)
        shifted = fixed + (places - fixed + offset_by * (used - fixed)) % max(1, amount - fixed)
        return jnp.zeros((amount,), jnp.int32).at[sequence[jnp.where(places < fixed, places, shifted)]].set(jnp.asarray(lengths, jnp.int32))

    lengths = jnp.where(number % 4 == 0, named(crowded, number // 4), named(usual, number - number // 4 - 1))
    mixed = jax.random.permutation(jax.random.fold_in(own, 3), amount)
    donor, taker = mixed[0:amount // 2 * 2:2], mixed[1:amount // 2 * 2:2]
    slack = jnp.minimum(lengths[donor] - 1, reach - lengths[taker]) // 2
    slack = jnp.where((donor == sequence[0]) | (taker == sequence[0]) | (lengths[taker] == 0), 0, jnp.maximum(slack, 0))
    shifted = jax.random.randint(jax.random.fold_in(own, 4), (amount // 2,), 0, 1 << 20) % (slack + 1)
    lengths = lengths.at[donor].add(-shifted).at[taker].add(shifted)
    members = jnp.searchsorted(jnp.cumsum(lengths), jnp.arange(rows * top), side="right").astype(jnp.int32)
    table = members.reshape(top, rows).T
    table = table[jax.random.permutation(jax.random.fold_in(own, 1), rows)]
    offset_by = jax.random.randint(jax.random.fold_in(own, 2), (rows, 1), 0, top)
    return jnp.take_along_axis(table, (jnp.arange(top)[None, :] + offset_by) % top, axis=1)


def portions_of(count, total, limit, lean, full):
    loads = [(1 << 20) // math.isqrt(standing ** lean) + 1 for standing in range(1, count + 1)]
    largest = limit if full else min(limit, max(-(-total // count), total * loads[0] // sum(loads)))
    least = 1 if total - largest >= count - 1 else 0
    holding, surplus = [largest] + [least] * (count - 1), total - largest - least * (count - 1)
    while surplus > 0:
        movable = [i for i in range(1, count) if holding[i] < largest] or [i for i in range(1, count) if holding[i] < limit]
        whole, remaining = sum([loads[i] for i in movable]), surplus
        for i in movable:
            extra = min(limit - holding[i], max(1, remaining * loads[i] // whole), surplus)
            holding[i] = holding[i] + extra
            surplus = surplus - extra
    return np.array(holding)


def gaussian(stream_key, shape, deviation, limit, shards=(), kind=jnp.bfloat16):
    result = jax.random.normal(stream_key, shape, jnp.float32) * deviation
    if len(shards) > 0:
        result = block_scale(stream_key, shape, shards, -0.22, 0.18) * result
    return jnp.clip(result, min=-limit, max=limit).astype(kind)


def heavy_noise(key, extent, width, limit, shards, heavy, held_as=jnp.bfloat16):
    result = width * jax.random.normal(key, extent, jnp.float32)
    if shards:
        result = result * block_scale(key, extent, shards, -0.22, 0.18)
    return jnp.clip(spiked(result, jax.random.fold_in(key, 3), *heavy), -limit, limit).astype(held_as)


def setup_inputs(seed: int = 0) -> dict:
    arg_keys = jax.random.split(jax.random.key(seed), 13)
    cotangent = heavy_noise(arg_keys[0], (TOKENS, D), 1.0, 6.0, ((0, 32),), (0, 1, 32, 2.75))
    mixer_out = gaussian(arg_keys[1], (TOKENS, D), 1.0, 6.0, ((0, 32),))
    expert_ids_keys = jax.random.split(jax.random.fold_in(arg_keys[2], 1), TOKENS // TOK_DEV)
    expert_ids_turns = jax.random.permutation(jax.random.fold_in(arg_keys[2], 3), TOKENS // TOK_DEV)
    expert_ids = jax.vmap(lambda own, number: deal_out(jax.random.fold_in(arg_keys[2], 2), own, number, TOK_DEV, EXPERTS, TOPK, CAP, 1))(expert_ids_keys, expert_ids_turns).reshape((TOKENS, TOPK))
    route_weight = jnp.clip(0.3 + 1.2 * jax.random.uniform(arg_keys[3], (TOKENS, TOPK), jnp.float32) ** block_scale(arg_keys[3], (TOKENS, TOPK), ((0, 32),), -0.2, 0.2), 0.3, 1.5)
    saved_normalized = gaussian(arg_keys[4], (TOKENS, CHANNELS), 1.0, 6.0, ((0, 32), (1, 16)))
    inverse_deviation = jnp.clip(jnp.exp(math.log(3.0) - 2.3025851 * jax.random.uniform(arg_keys[5], (TOKENS,), jnp.float32) ** block_scale(arg_keys[5], (TOKENS,), ((0, 32),), -0.2, 0.2)), 0.3, 3.0)
    channel_norm_gain = jnp.clip(1.0 + 0.18 * jax.random.normal(arg_keys[6], (CHANNELS,), jnp.float32), 0.1, 1.9)
    taps = gaussian(arg_keys[7], (WIDTH, CHANNELS), 0.18, 1.0, ((1, 16),), jnp.float32)
    proj_weight = gaussian(arg_keys[8], (CHANNELS, D), CHANNELS ** -0.5, 0.125, ((0, 16),))
    gate_weight = gaussian(arg_keys[9], (EXPERTS, D, EXPERT_FF), D ** -0.5, 0.125, ((0, 32), (2, 16)))
    up_weight = gaussian(arg_keys[10], (EXPERTS, D, EXPERT_FF), D ** -0.5, 0.125, ((0, 32), (2, 16)))
    down_weight = gaussian(arg_keys[11], (EXPERTS, EXPERT_FF, D), EXPERT_FF ** -0.5, 0.125, ((0, 32), (1, 16)))
    return dict(cotangent=cotangent, mixer_out=mixer_out, expert_ids=expert_ids, route_weight=route_weight, saved_normalized=saved_normalized, inverse_deviation=inverse_deviation, channel_norm_gain=channel_norm_gain, taps=taps, proj_weight=proj_weight, gate_weight=gate_weight, up_weight=up_weight, down_weight=down_weight)


def expert_pass(operands):
    routed_rows, routed_grad, w_first, w_third, w_second = operands
    hidden_gate = jnp.dot(routed_rows, w_first, preferred_element_type=jnp.float32)
    hidden_up = jnp.dot(routed_rows, w_third, preferred_element_type=jnp.float32)
    sigma = jax.nn.sigmoid(hidden_gate)
    swish = hidden_gate * sigma
    activ = (swish * hidden_up).astype(jnp.bfloat16)
    grad_second = jnp.dot(activ.T, routed_grad, preferred_element_type=jnp.float32).astype(jnp.bfloat16)
    grad_activ = jnp.dot(routed_grad, w_second.T, preferred_element_type=jnp.float32)
    grad_gpre = (grad_activ * hidden_up * sigma * (1.0 + hidden_gate * (1.0 - sigma))).astype(jnp.bfloat16)
    grad_upre = (grad_activ * swish).astype(jnp.bfloat16)
    grad_first = jnp.dot(routed_rows.T, grad_gpre, preferred_element_type=jnp.float32).astype(jnp.bfloat16)
    grad_third = jnp.dot(routed_rows.T, grad_upre, preferred_element_type=jnp.float32).astype(jnp.bfloat16)
    slot_count = routed_rows.shape[0]
    model_width = routed_rows.shape[1]
    split_gate = grad_gpre.astype(jnp.float32).reshape(slot_count, N_TP, FFD)
    split_upre = grad_upre.astype(jnp.float32).reshape(slot_count, N_TP, FFD)
    first_split = w_first.astype(jnp.float32).reshape(model_width, N_TP, FFD)
    third_split = w_third.astype(jnp.float32).reshape(model_width, N_TP, FFD)
    partial_value = jnp.einsum('rgf,dgf->grd', split_gate, first_split) + jnp.einsum('rgf,dgf->grd', split_upre, third_split)
    rounded = lax.optimization_barrier(partial_value.astype(jnp.bfloat16))
    slot_grad = jnp.sum(rounded.astype(jnp.float32), axis=0).astype(jnp.bfloat16)
    return grad_first, grad_third, grad_second, slot_grad


def reference(cotangent, mixer_out, expert_ids, route_weight, saved_normalized, inverse_deviation, channel_norm_gain, taps,
              proj_weight, gate_weight, up_weight, down_weight):
    onehot = (expert_ids[:, :, None] == jnp.arange(EXPERTS, dtype=jnp.int32)[None, None, :]).astype(jnp.int32)
    flat_hot = onehot.reshape(N_SP, TOK_DEV * TOPK, EXPERTS)
    ranks = jnp.cumsum(flat_hot, axis=1) - flat_hot
    rank_pair = jnp.sum(ranks * flat_hot, axis=2).reshape(TOKENS, TOPK)
    block_index = (jnp.arange(TOKENS, dtype=jnp.int32) // TOK_DEV)[:, None]
    position = (expert_ids * (N_SP * CAP) + block_index * CAP + rank_pair).reshape(-1).astype(jnp.int32)
    rows_pair = jnp.broadcast_to(mixer_out[:, None, :], (TOKENS, TOPK, D)).reshape(-1, D)
    grad_pair = (route_weight[:, :, None] * cotangent.astype(jnp.float32)[:, None, :]).astype(jnp.bfloat16).reshape(-1, D)
    row_buffer = jnp.zeros((EXPERTS * N_SP * CAP, D), jnp.bfloat16).at[position].set(rows_pair)
    grad_buffer = jnp.zeros((EXPERTS * N_SP * CAP, D), jnp.bfloat16).at[position].set(grad_pair)
    row_buffer = row_buffer.reshape(EXPERTS, N_SP * CAP, D)
    grad_buffer = grad_buffer.reshape(EXPERTS, N_SP * CAP, D)
    grad_gate, grad_up, grad_down, slot_grad = lax.map(
        expert_pass, (row_buffer, grad_buffer, gate_weight, up_weight, down_weight))
    returned = slot_grad.reshape(-1, D)[position].reshape(TOKENS, TOPK, D).astype(jnp.float32)
    mixer_grad = (cotangent.astype(jnp.float32) + jnp.sum(returned, axis=1)).astype(jnp.bfloat16)

    normalized_values = saved_normalized.astype(jnp.float32) * channel_norm_gain[None, :]
    sigma = jax.nn.sigmoid(normalized_values)
    act_conv = (normalized_values * sigma).astype(jnp.bfloat16)
    grad_proj = jnp.dot(mixer_grad.T, act_conv, preferred_element_type=jnp.float32)
    grad_act = jnp.dot(mixer_grad, proj_weight.T, preferred_element_type=jnp.float32)
    norm_output_gradient = grad_act * sigma * (1.0 + normalized_values * (1.0 - sigma)) * channel_norm_gain[None, :]
    normalized_input = saved_normalized.astype(jnp.float32)
    gradient_mean = jnp.mean(norm_output_gradient, axis=1, keepdims=True)
    projected_mean = jnp.mean(norm_output_gradient * normalized_input, axis=1, keepdims=True)
    conv_output_gradient = inverse_deviation[:, None] * (norm_output_gradient - gradient_mean - normalized_input * projected_mean)
    padded = jnp.concatenate([conv_output_gradient, jnp.zeros((WIDTH - 1, CHANNELS), jnp.float32)], axis=0)
    total = jnp.zeros((TOKENS, CHANNELS), jnp.float32)
    for tap_index in range(WIDTH):
        total = total + taps[tap_index][None, :] * padded[tap_index:tap_index + TOKENS]
    return total.astype(jnp.bfloat16), grad_proj, grad_gate, grad_up, grad_down
```

```python
import jax
import jax.numpy as jnp
from jax import lax
from jax.sharding import Mesh, PartitionSpec as P

BF, F32 = jnp.bfloat16, jnp.float32
SWAP = [(0, 1), (1, 0)]
LAST = (((1,), (1,)), ((), ()))
FIRST = (((0,), (0,)), ((), ()))


def mm(a, b, dims=(((1,), (0,)), ((), ()))):
    return lax.dot_general(a, b, dims, preferred_element_type=F32)


def flip_y(value, bit):
    return lax.ppermute(value, "y", [(i, i ^ bit) for i in range(lax.axis_size("y"))])


def flip_c(value):
    return lax.ppermute(value, "c", SWAP)


def shards(
    cotangent,
    mixer_out,
    expert_ids,
    route_weight,
    saved_normalized,
    inverse_deviation,
    channel_norm_gain,
    taps,
    proj_weight,
    gate_weight,
    up_weight,
    down_weight,
):
    sp = ("z", "x")
    experts = lax.axis_size(sp)
    ny = lax.axis_size("y")
    yi, ci = lax.axis_index("y"), lax.axis_index("c")
    tok, width = cotangent.shape
    span = 4
    group = (yi % 2) * 2 + ci
    own = (gate_weight[0], up_weight[0], down_weight[0])

    by_c = tuple(flip_c(w) for w in own)
    by_y = tuple(flip_y(w, 1) for w in own)
    by_yc = tuple(flip_c(w) for w in by_y)

    lane_e = jnp.arange(experts, dtype=jnp.int32)[None, :]
    hot = [(expert_ids[:, k : k + 1] == lane_e) for k in range(2)]
    both = (hot[0] | hot[1]).astype(BF)
    before = (
        jnp.arange(tok, dtype=jnp.int32)[:, None] > jnp.arange(tok, dtype=jnp.int32)[None, :]
    ).astype(BF)
    rank = mm(before, both)
    slot_of = jnp.where(both > 0, rank, -1.0)
    targets = group * span + jnp.arange(span, dtype=jnp.int32)
    picked = slot_of.T[:, None, :] == targets.astype(F32)[None, :, None]
    dispatch = picked.astype(BF).reshape(experts * span, tok)
    wte = sum(jnp.where(hot[k], route_weight[:, k : k + 1], 0.0) for k in range(2))
    slot_weight = jnp.sum(jnp.where(picked, wte.T[:, None, :], 0.0), axis=2)
    rows = mm(dispatch, mixer_out).astype(BF).reshape(experts, span, width)
    grads = (slot_weight.reshape(-1, 1) * mm(dispatch, cotangent)).astype(BF)
    sent = jnp.concatenate([rows, grads.reshape(experts, span, width)], axis=1)
    got = lax.all_to_all(sent, sp, 0, 0, tiled=True)
    x = got[:, :span].reshape(-1, width)
    g = got[:, span:].reshape(-1, width)

    col = jnp.arange(ny * 2 * span, dtype=jnp.int32)
    col_y, col_h, col_r = col // (2 * span), (col // span) % 2, col % span
    col_rank = ((col_y % 2) * 2 + ci) * span + col_r
    hit = (slot_of[:, :, None] == col_rank.astype(F32)[None, None, :])
    halves = jnp.stack([ci, 1 - ci])
    table = (hit[None] & (col_h[None, :] == halves[:, None])[:, None, None, :]).astype(BF)
    table = table.reshape(2 * tok, -1)

    hidden = []
    partial = jnp.zeros((x.shape[0], width), F32)
    for w1, w3, w2 in (own, by_c, by_y, by_yc):
        hg, hu = mm(x, w1), mm(x, w3)
        sigma = jax.nn.sigmoid(hg)
        swish = hg * sigma
        act = (swish * hu).astype(BF)
        gact = mm(g, w2, LAST)
        ghg = (gact * hu * sigma * (1.0 + hg * (1.0 - sigma))).astype(BF)
        ghu = (gact * swish).astype(BF)
        partial = partial + mm(ghg, w1, LAST) + mm(ghu, w3, LAST)
        hidden.append((act, ghg, ghu))
    back = partial.astype(BF).reshape(experts, span, ny, 2, 128)
    back = back.transpose(0, 2, 3, 1, 4).reshape(experts * ny, 2 * span, 128)
    home = lax.all_to_all(back, ("z", "x", "y"), 0, 0, tiled=True).reshape(-1, 128)

    def weight_grads(q):
        act, ghg, ghu = hidden[q]
        return mm(x, ghg, FIRST), mm(x, ghu, FIRST), mm(act, g, FIRST)

    mine, theirs_c, mine_y, theirs_yc = (weight_grads(q) for q in range(4))
    final = []
    for a, b, o, p in zip(mine, mine_y, theirs_c, theirs_yc):
        a = a + flip_c(o.astype(BF)).astype(F32)
        b = b + flip_c(p.astype(BF)).astype(F32)
        final.append((a + flip_y(b.astype(BF), 1).astype(F32)).astype(BF))

    combined = mm(table, home)
    other = flip_c(combined[tok:].astype(BF))
    feat = (yi * 2 + ci) * 128
    cot = lax.dynamic_slice_in_dim(cotangent, feat, 128, axis=1)
    mix = (cot.astype(F32) + combined[:tok] + other.astype(F32)).astype(BF)
    mine_all = lax.all_to_all(jnp.broadcast_to(mix[None], (ny, *mix.shape)), "y", 0, 0, tiled=True)
    other_all = flip_c(mine_all)
    first = jnp.where(ci == 0, mine_all, other_all)
    second = jnp.where(ci == 0, other_all, mine_all)
    mixer_grad = jnp.stack([first, second], axis=1).transpose(2, 0, 1, 3).reshape(tok, width)

    normalized = saved_normalized.astype(F32)
    values = normalized * channel_norm_gain[None, :]
    gate = jax.nn.sigmoid(values)
    act_conv = (values * gate).astype(BF)
    slope = gate * (1.0 + values * (1.0 - gate)) * channel_norm_gain[None, :]
    proj = mm(mixer_grad, act_conv, FIRST).astype(BF).reshape(experts, -1, 128)
    proj = lax.all_to_all(proj, sp, 0, 0, tiled=True)
    grad_proj = jnp.sum(proj.astype(F32), axis=0)

    grad_norm = mm(mixer_grad, proj_weight, LAST) * slope
    sums = jnp.stack([jnp.sum(grad_norm, axis=1), jnp.sum(grad_norm * normalized, axis=1)])
    sums = sums + flip_c(sums)
    for bit in (1, 2, 4):
        sums = sums + flip_y(sums, bit)
    mean = sums / (128 * 2 * ny)
    conv = inverse_deviation[:, None] * (
        grad_norm - mean[0][:, None] - normalized * mean[1][:, None]
    )
    reach = taps.shape[0] - 1
    beyond = lax.ppermute(conv[:reach], sp, [(i + 1, i) for i in range(experts - 1)])
    extended = jnp.concatenate([conv, beyond], axis=0)
    result = jnp.zeros_like(conv)
    for j in range(reach + 1):
        result = result + taps[j][None, :] * extended[j : j + tok]
    return (result.astype(BF), grad_proj, final[0][None], final[1][None], final[2][None])


def solution(mesh):
    fine = Mesh(mesh.devices.reshape(8, 4, 8, 2), ("z", "x", "y", "c"))
    sp, tp = ("z", "x"), ("y", "c")
    return jax.shard_map(
        shards,
        mesh=fine,
        in_specs=(
            P(sp, None),
            P(sp, None),
            P(sp, None),
            P(sp, None),
            P(sp, tp),
            P(sp),
            P(tp),
            P(None, tp),
            P(tp, None),
            P(sp, None, tp),
            P(sp, None, tp),
            P(sp, tp, None),
        ),
        out_specs=(
            P(sp, tp),
            P(sp, tp),
            P(sp, None, tp),
            P(sp, None, tp),
            P(sp, tp, None),
        ),
        check_vma=False,
    )
```

```python
import jax
import jax.numpy as jnp
from jax import lax
from jax.experimental import pallas as pl
from jax.experimental.pallas import tpu as pltpu
from jax.sharding import Mesh, PartitionSpec as P

BF, F32, I32 = jnp.bfloat16, jnp.float32, jnp.int32
LAST = (((1,), (1,)), ((), ()))
FIRST = (((0,), (0,)), ((), ()))
SPAN = 4
VMEM = pl.BlockSpec(memory_space=pltpu.VMEM)


def mm(a, b, dims=(((1,), (0,)), ((), ()))):
    return lax.dot_general(a, b, dims, preferred_element_type=F32)


def iota(shape, dim):
    return lax.broadcasted_iota(I32, shape, dim)


def kernel(body, outs, flops, *args):
    return pl.pallas_call(
        body,
        out_shape=outs,
        in_specs=[VMEM] * len(args),
        out_specs=jax.tree.map(lambda _: VMEM, outs),
        cost_estimate=pl.CostEstimate(flops=flops, bytes_accessed=1 << 20, transcendentals=0),
    )(*args)


def shape(*dims, kind=BF):
    return jax.ShapeDtypeStruct(dims, kind)


def head_body(ids_ref, weight_ref, mix_ref, cot_ref, out_ref):
    tok = ids_ref.shape[0]
    experts = out_ref.shape[0] // (2 * SPAN)
    group = (lax.axis_index("y") % 2) * 2 + lax.axis_index("c")
    ids = [jnp.broadcast_to(ids_ref[:, k : k + 1], (tok, tok)).T[:1] for k in range(2)]
    wts = [jnp.broadcast_to(weight_ref[:, k : k + 1], (tok, tok)).T[:1] for k in range(2)]
    expert = iota((experts, tok), 0)
    hot = [(expert == i).astype(F32) for i in ids]
    after = (iota((tok, tok), 0) < iota((tok, tok), 1)).astype(BF)
    rank = mm((hot[0] + hot[1]).astype(BF), after)
    rows = out_ref.shape[0]
    row = iota((rows, tok), 0)
    row_e, row_j = row // (2 * SPAN), row % (2 * SPAN)
    target = group * SPAN + row_j % SPAN
    found = jnp.zeros((rows, tok), jnp.bool_)
    scale = jnp.zeros((rows, tok), F32)
    for i, w, h in zip(ids, wts, hot):
        place = jnp.sum(rank * h, axis=0, keepdims=True).astype(I32)
        match = (row_e == i) & (target == place)
        found = found | match
        scale = jnp.where(match, w, scale)
    scale = jnp.sum(scale, axis=1, keepdims=True)
    is_x = row_j < SPAN
    take_x = jnp.where(found & is_x, 1.0, 0.0).astype(BF)
    take_g = jnp.where(found & ~is_x, 1.0, 0.0).astype(BF)
    scale = jnp.where(iota((rows, 1), 0) % (2 * SPAN) < SPAN, 1.0, scale)
    step = 512
    for at in range(0, mix_ref.shape[1], step):
        picked = mm(take_x, mix_ref[:, at : at + step]) + mm(take_g, cot_ref[:, at : at + step])
        out_ref[:, at : at + step] = (picked * scale).astype(BF)


def table_body(ids_ref, out_ref):
    tok = ids_ref.shape[0]
    ci = lax.axis_index("c")
    cols = out_ref.shape[1]
    experts = cols // 64
    lane = iota((tok, experts), 1)
    hot = jnp.zeros((tok, experts), F32)
    for k in range(2):
        hot = hot + (lane == ids_ref[:, k : k + 1]).astype(F32)
    before = (iota((tok, tok), 0) > iota((tok, tok), 1)).astype(BF)
    slot = jnp.where(hot > 0, mm(before, hot.astype(BF)), -1.0)
    spread = (iota((experts, cols), 1) // 64 == iota((experts, cols), 0)).astype(BF)
    held = mm(slot.astype(BF), spread).astype(I32)
    col = iota((tok, cols), 1)
    place = ((col // 8) % 2 * 2 + ci) * SPAN + col % SPAN
    half = (col // SPAN) % 2
    hit = held == place
    out_ref[:tok, :] = jnp.where(hit & (half == ci), 1.0, 0.0).astype(BF)
    out_ref[tok:, :] = jnp.where(hit & (half != ci), 1.0, 0.0).astype(BF)


def pack_body(gate_ref, up_ref, down_ref, out_ref):
    out_ref[0] = gate_ref[...]
    out_ref[1] = up_ref[...]
    for j in range(down_ref.shape[1] // 128):
        out_ref[2, j * 128 : (j + 1) * 128, :] = down_ref[:, j * 128 : (j + 1) * 128]


def expert_body(got_ref, w0, w1, w2, w3, x_ref, g_ref, hid_ref, back_ref):
    rows, width = got_ref.shape
    slots = rows // 2
    out_row, in_row = iota((slots, rows), 0), iota((slots, rows), 1)
    want = (out_row // SPAN) * (2 * SPAN) + out_row % SPAN
    pick_x = (in_row == want).astype(BF)
    pick_g = (in_row == want + SPAN).astype(BF)
    for at in range(0, width, 512):
        part = got_ref[:, at : at + 512]
        x_ref[:, at : at + 512] = mm(pick_x, part).astype(BF)
        g_ref[:, at : at + 512] = mm(pick_g, part).astype(BF)
    for q, w in enumerate((w0, w1, w2, w3)):
        hg = mm(x_ref[...], w[0])
        hu = mm(x_ref[...], w[1])
        gact = jnp.zeros((slots, 128), F32)
        for j in range(width // 128):
            gact = gact + mm(
                g_ref[:, j * 128 : (j + 1) * 128], w[2, j * 128 : (j + 1) * 128, :], LAST
            )
        sigma = jax.nn.sigmoid(hg)
        swish = hg * sigma
        lanes = slice(q * 128, (q + 1) * 128)
        hid_ref[0, :, lanes] = (gact * hu * sigma * (1.0 + hg * (1.0 - sigma))).astype(BF)
        hid_ref[1, :, lanes] = (gact * swish).astype(BF)
        hid_ref[2, :, lanes] = (swish * hu).astype(BF)
    low = iota((slots, 128), 0) % (2 * SPAN) < SPAN
    for y in range(width // 256):
        pair = []
        for h in range(2):
            at = (y * 2 + h) * 128
            acc = jnp.zeros((slots, 128), F32)
            for q, w in enumerate((w0, w1, w2, w3)):
                lanes = slice(q * 128, (q + 1) * 128)
                acc = acc + mm(hid_ref[0, :, lanes], w[0, at : at + 128, :], LAST)
                acc = acc + mm(hid_ref[1, :, lanes], w[1, at : at + 128, :], LAST)
            pair.append(acc)
        even = jnp.where(low, pair[0], pltpu.roll(pair[1], SPAN, 0))
        odd = jnp.where(low, pltpu.roll(pair[0], slots - SPAN, 0), pair[1])
        back_ref[:, y * 8 : (y + 1) * 8, :] = even.reshape(-1, 8, 128).astype(BF)
        back_ref[:, 64 + y * 8 : 64 + (y + 1) * 8, :] = odd.reshape(-1, 8, 128).astype(BF)


def grads_body(x_ref, g_ref, hid_ref, keep_ref, give_ref):
    width = x_ref.shape[1]
    for j in range(width // 128):
        at = slice(j * 128, (j + 1) * 128)
        xt, gt = x_ref[:, at], g_ref[:, at]
        for m in range(3):
            h = hid_ref[m]
            both = mm(xt, h, FIRST) if m < 2 else mm(h, gt, FIRST)
            for q in range(4):
                ref, to = ((keep_ref, 0), (give_ref, 0), (keep_ref, 1), (give_ref, 1))[q]
                cut = slice(q * 128, (q + 1) * 128)
                piece = both[:, cut] if m < 2 else both[cut, :]
                ref[to, m, at, :] = piece.astype(BF)


def final_body(mine_ref, other_ref, proj_ref, act_ref, slope_ref, norm_ref, out_ref, grad_ref, sum_ref):
    ci = lax.axis_index("c")
    tok = act_ref.shape[0]
    acc = jnp.zeros((tok, tok), F32)
    for y in range(mine_ref.shape[0]):
        for ref, cc in ((mine_ref, ci), (other_ref, 1 - ci)):
            at = pl.ds(pl.multiple_of((2 * y + cc) * 128, 128), 128)
            part = ref[y]
            out_ref[at, :] = mm(part, act_ref[...], FIRST).astype(BF)
            acc = acc + mm(part, proj_ref[:, at], LAST)
    grad = acc * slope_ref[...]
    grad_ref[...] = grad
    sum_ref[0:1, :] = jnp.sum(grad.T, axis=0, keepdims=True)
    sum_ref[1:2, :] = jnp.sum((grad * norm_ref[...]).T, axis=0, keepdims=True)


def shards(
    cotangent,
    mixer_out,
    expert_ids,
    route_weight,
    saved_normalized,
    inverse_deviation,
    channel_norm_gain,
    taps,
    proj_weight,
    gate_weight,
    up_weight,
    down_weight,
):
    sp = ("z", "x")
    experts = lax.axis_size(sp)
    ny = lax.axis_size("y")
    yi, ci = lax.axis_index("y"), lax.axis_index("c")
    tok, width = cotangent.shape

    def flip_c(value):
        return lax.ppermute(value, "c", [(0, 1), (1, 0)])

    def hop(value, sign):
        pairs = []
        for y in range(ny):
            for c in range(2):
                pairs.append((2 * y + c, 2 * ((y + (sign if c == 0 else -sign)) % ny) + c))
        return lax.ppermute(value, ("y", "c"), pairs)

    own = kernel(pack_body, shape(3, width, 128), 1000000, gate_weight[0], up_weight[0], down_weight[0])
    by_y = hop(own, 1)
    by_c = flip_c(own)
    by_yc = flip_c(by_y)

    rows = experts * 2 * SPAN
    sent = kernel(
        head_body, shape(rows, width), 2000000000, expert_ids, route_weight, mixer_out, cotangent
    )
    got = lax.all_to_all(sent.reshape(experts, 2 * SPAN, width), sp, 0, 0, tiled=True)
    table = kernel(table_body, shape(2 * tok, experts * ny * 2 * SPAN), 2000000000, expert_ids)

    normalized = saved_normalized.astype(F32)
    values = normalized * channel_norm_gain[None, :]
    gate = jax.nn.sigmoid(values)
    act_conv = (values * gate).astype(BF)
    slope = gate * (1.0 + values * (1.0 - gate)) * channel_norm_gain[None, :]

    slots = experts * SPAN
    x, g, hidden, back = kernel(
        expert_body,
        (shape(slots, width), shape(slots, width), shape(3, slots, 512), shape(experts // 2, 128, 128)),
        4000000000,
        got.reshape(rows, width),
        own,
        by_c,
        by_y,
        by_yc,
    )
    home = lax.all_to_all(
        back.reshape(experts * ny, 2 * SPAN, 128), ("z", "x", "y"), 0, 0, tiled=True
    ).reshape(-1, 128)

    packed = shape(2, 3, width, 128)
    keep, give = kernel(grads_body, (packed, packed), 8000000000, x, g, hidden)
    given = flip_c(give)
    passed = hop((keep[1].astype(F32) + given[1].astype(F32)).astype(BF), -1)
    final = (keep[0].astype(F32) + given[0].astype(F32) + passed.astype(F32)).astype(BF)
    grad_down = final[2].reshape(-1, 128, 128).transpose(1, 0, 2).reshape(128, width)

    combined = mm(table, home)
    other = flip_c(combined[tok:].astype(BF))
    feat = (yi * 2 + ci) * 128
    cot = lax.dynamic_slice_in_dim(cotangent, feat, 128, axis=1)
    mix = (cot.astype(F32) + combined[:tok] + other.astype(F32)).astype(BF)
    mine_all = lax.all_to_all(jnp.broadcast_to(mix[None], (ny, *mix.shape)), "y", 0, 0, tiled=True)
    other_all = flip_c(mine_all)

    proj, grad_norm, sums = kernel(
        final_body,
        (shape(width, 128), shape(tok, 128, kind=F32), shape(2, 128, kind=F32)),
        2000000000,
        mine_all,
        other_all,
        proj_weight,
        act_conv,
        slope,
        normalized,
    )
    proj = lax.all_to_all(proj.reshape(experts, -1, 128), sp, 0, 0, tiled=True)
    grad_proj = jnp.sum(proj.astype(F32), axis=0)

    sums = sums + flip_c(sums)
    for bit in (1, 2, 4):
        sums = sums + lax.ppermute(sums, "y", [(i, i ^ bit) for i in range(ny)])
    mean = sums / (128 * 2 * ny)
    conv = inverse_deviation[:, None] * (
        grad_norm - mean[0][:, None] - normalized * mean[1][:, None]
    )
    reach = taps.shape[0] - 1
    beyond = lax.ppermute(conv[:reach], sp, [(i + 1, i) for i in range(experts - 1)])
    extended = jnp.concatenate([conv, beyond], axis=0)
    result = jnp.zeros_like(conv)
    for j in range(reach + 1):
        result = result + taps[j][None, :] * extended[j : j + tok]
    return (result.astype(BF), grad_proj, final[0][None], final[1][None], grad_down[None])


def solution(mesh):
    fine = Mesh(mesh.devices.reshape(8, 4, 8, 2), ("z", "x", "y", "c"))
    sp, tp = ("z", "x"), ("y", "c")
    return jax.shard_map(
        shards,
        mesh=fine,
        in_specs=(
            P(sp, None),
            P(sp, None),
            P(sp, None),
            P(sp, None),
            P(sp, tp),
            P(sp),
            P(tp),
            P(None, tp),
            P(tp, None),
            P(sp, None, tp),
            P(sp, None, tp),
            P(sp, tp, None),
        ),
        out_specs=(
            P(sp, tp),
            P(sp, tp),
            P(sp, None, tp),
            P(sp, None, tp),
            P(sp, tp, None),
        ),
        check_vma=False,
    )
```

```python
import jax
import jax.numpy as jnp
from jax import lax
from jax.experimental import pallas as pl
from jax.experimental.pallas import tpu as pltpu
from jax.sharding import Mesh, PartitionSpec as P


BF, F32, I32 = jnp.bfloat16, jnp.float32, jnp.int32
LAST = (((1,), (1,)), ((), ()))
FIRST = (((0,), (0,)), ((), ()))
SPAN = 4
VMEM = pl.BlockSpec(memory_space=pltpu.VMEM)
ANY = pl.BlockSpec(memory_space=pl.ANY)


def mm(a, b, dims=(((1,), (0,)), ((), ()))):
    return lax.dot_general(a, b, dims, preferred_element_type=F32)


def iota(shape, dim):
    return lax.broadcasted_iota(I32, shape, dim)


def kernel(body, outs, flops, *args, scratch=(), far=()):
    return pl.pallas_call(
        body,
        out_shape=outs,
        in_specs=[ANY if i in far else VMEM for i in range(len(args))],
        scratch_shapes=list(scratch),
        out_specs=jax.tree.map(lambda _: VMEM, outs),
        cost_estimate=pl.CostEstimate(flops=flops, bytes_accessed=1 << 20, transcendentals=0),
    )(*args)


def shape(*dims, kind=BF):
    return jax.ShapeDtypeStruct(dims, kind)


def head_body(ids_ref, weight_ref, mix_ref, cot_ref, out_ref):
    tok = ids_ref.shape[1]
    experts = out_ref.shape[0] // (2 * SPAN)
    group = (lax.axis_index("y") % 2) * 2 + lax.axis_index("c")
    ids = [ids_ref[k : k + 1, :] for k in range(2)]
    wts = [weight_ref[k : k + 1, :] for k in range(2)]
    expert = iota((experts, tok), 0)
    hot = [(expert == i).astype(F32) for i in ids]
    after = (iota((tok, tok), 0) < iota((tok, tok), 1)).astype(BF)
    rank = mm((hot[0] + hot[1]).astype(BF), after)
    rows = out_ref.shape[0]
    row = iota((rows, tok), 0)
    row_e, row_j = row // (2 * SPAN), row % (2 * SPAN)
    target = group * SPAN + row_j % SPAN
    found = jnp.zeros((rows, tok), jnp.bool_)
    scale = jnp.zeros((rows, tok), F32)
    for i, w, h in zip(ids, wts, hot):
        place = jnp.sum(rank * h, axis=0, keepdims=True).astype(I32)
        match = (row_e == i) & (target == place)
        found = found | match
        scale = jnp.where(match, w, scale)
    scale = jnp.sum(scale, axis=1, keepdims=True)
    is_x = row_j < SPAN
    take_x = jnp.where(found & is_x, 1.0, 0.0).astype(BF)
    take_g = jnp.where(found & ~is_x, 1.0, 0.0).astype(BF)
    scale = jnp.where(iota((rows, 1), 0) % (2 * SPAN) < SPAN, 1.0, scale)
    step = 512
    for at in range(0, mix_ref.shape[1], step):
        picked = mm(take_x, mix_ref[:, at : at + step]) + mm(take_g, cot_ref[:, at : at + step])
        out_ref[:, at : at + step] = (picked * scale).astype(BF)


def table_body(ids_ref, out_ref):
    tok = ids_ref.shape[1]
    ci = lax.axis_index("c")
    cols = out_ref.shape[1]
    experts = cols // 64
    lane = iota((tok, experts), 1)
    hot = jnp.zeros((tok, experts), F32)
    for k in range(2):
        ids = jnp.broadcast_to(ids_ref[k : k + 1, :].astype(F32), (tok, tok)).T
        hot = hot + (lane == ids[:, :experts].astype(I32)).astype(F32)
    before = (iota((tok, tok), 0) > iota((tok, tok), 1)).astype(BF)
    slot = jnp.where(hot > 0, mm(before, hot.astype(BF)), -1.0)
    spread = (iota((experts, cols), 1) // 64 == iota((experts, cols), 0)).astype(BF)
    held = mm(slot.astype(BF), spread).astype(I32)
    col = iota((tok, cols), 1)
    place = ((col // 8) % 2 * 2 + ci) * SPAN + col % SPAN
    half = (col // SPAN) % 2
    hit = held == place
    out_ref[:tok, :] = jnp.where(hit & (half == ci), 1.0, 0.0).astype(BF)
    out_ref[tok:, :] = jnp.where(hit & (half != ci), 1.0, 0.0).astype(BF)


def pack_body(gate_ref, up_ref, down_ref, out_ref):
    out_ref[0] = gate_ref[...]
    out_ref[1] = up_ref[...]
    for j in range(down_ref.shape[1] // 128):
        out_ref[2, j * 128 : (j + 1) * 128, :] = down_ref[:, j * 128 : (j + 1) * 128]


def expert_body(got_ref, w0, w1, w2, w3, x_ref, g_ref, hid_ref, back_ref, in_ref, down_ref, sem):
    rows, width = got_ref.shape
    slots = rows // 2
    copies = []
    for q, w in enumerate((w0, w1, w2, w3)):
        three = []
        for m in range(2):
            at = (2 * q + m) * 128
            three.append(pltpu.make_async_copy(w.at[m], in_ref.at[:, at : at + 128], sem.at[q, m]))
        down = w.at[2].reshape(width // 128, 128, 128)
        three.append(
            pltpu.make_async_copy(down, down_ref.at[:, q * 128 : (q + 1) * 128, :], sem.at[q, 2])
        )
        for copy in three:
            copy.start()
        copies.append(three)
    out_row, in_row = iota((slots, rows), 0), iota((slots, rows), 1)
    want = (out_row // SPAN) * (2 * SPAN) + out_row % SPAN
    pick_x = (in_row == want).astype(BF)
    pick_g = (in_row == want + SPAN).astype(BF)
    for at in range(0, width, 512):
        part = got_ref[:, at : at + 512]
        x_ref[:, at : at + 512] = mm(pick_x, part).astype(BF)
        g_ref[:, at : at + 512] = mm(pick_g, part).astype(BF)
    for q in range(4):
        for copy in copies[q]:
            copy.wait()
        both = mm(x_ref[...], in_ref[:, q * 256 : (q + 1) * 256])
        hg, hu = both[:, :128], both[:, 128:]
        gact = jnp.zeros((slots, 128), F32)
        for j in range(0, width // 128, 2):
            blocks = [down_ref[j + i, q * 128 : (q + 1) * 128, :] for i in range(2)]
            gact = gact + mm(
                g_ref[:, j * 128 : (j + 2) * 128], jnp.concatenate(blocks, axis=1), LAST
            )
        sigma = jax.nn.sigmoid(hg)
        swish = hg * sigma
        at = q * 256
        hid_ref[:, at : at + 128] = (gact * hu * sigma * (1.0 + hg * (1.0 - sigma))).astype(BF)
        hid_ref[:, at + 128 : at + 256] = (gact * swish).astype(BF)
        hid_ref[:, 1024 + q * 128 : 1152 + q * 128] = (swish * hu).astype(BF)
    low = iota((slots, 128), 0) % (2 * SPAN) < SPAN
    for y in range(width // 256):
        both = mm(hid_ref[:, :1024], in_ref[y * 256 : (y + 1) * 256, :], LAST)
        pair = [both[:, :128], both[:, 128:]]
        even = jnp.where(low, pair[0], pltpu.roll(pair[1], SPAN, 0))
        odd = jnp.where(low, pltpu.roll(pair[0], slots - SPAN, 0), pair[1])
        back_ref[:, y * 8 : (y + 1) * 8, :] = even.reshape(-1, 8, 128).astype(BF)
        back_ref[:, 64 + y * 8 : 64 + (y + 1) * 8, :] = odd.reshape(-1, 8, 128).astype(BF)


def grads_body(x_ref, g_ref, hid_ref, keep_ref, give_ref):
    width = x_ref.shape[1]
    places = ((keep_ref, 0), (give_ref, 0), (keep_ref, 1), (give_ref, 1))
    for j in range(width // 128):
        at = slice(j * 128, (j + 1) * 128)
        both = mm(x_ref[:, at], hid_ref[:, :1024], FIRST)
        down = mm(hid_ref[:, 1024:], g_ref[:, at], FIRST)
        for q, (ref, to) in enumerate(places):
            ref[to, 0, at, :] = both[:, q * 256 : q * 256 + 128].astype(BF)
            ref[to, 1, at, :] = both[:, q * 256 + 128 : (q + 1) * 256].astype(BF)
            ref[to, 2, at, :] = down[q * 128 : (q + 1) * 128, :].astype(BF)


def combine_body(table_ref, home_ref, cot_ref, own_ref, other_ref):
    tok = cot_ref.shape[0]
    place = lax.axis_index("y") * 2 + lax.axis_index("c")
    cot = cot_ref[:, pl.ds(pl.multiple_of(place * 128, 128), 128)].astype(F32)
    both = mm(table_ref[...], home_ref[...])
    own_ref[...] = both[:tok] + cot
    other_ref[...] = both[tok:].astype(BF)


def mix_body(own_ref, other_ref, out_ref):
    mix = (own_ref[...] + other_ref[...].astype(F32)).astype(BF)
    for y in range(out_ref.shape[0]):
        out_ref[y] = mix


def final_body(mine_ref, other_ref, proj_ref, act_ref, slope_ref, norm_ref, out_ref, grad_ref, sum_ref):
    ci = lax.axis_index("c")
    tok = act_ref.shape[0]
    acc = jnp.zeros((tok, tok), F32)
    for y in range(mine_ref.shape[0]):
        for ref, cc in ((mine_ref, ci), (other_ref, 1 - ci)):
            at = pl.ds(pl.multiple_of((2 * y + cc) * 128, 128), 128)
            part = ref[y]
            out_ref[at, :] = mm(part, act_ref[...], FIRST).astype(BF)
            acc = acc + mm(part, proj_ref[:, at], LAST)
    grad = acc * slope_ref[...]
    grad_ref[...] = grad
    sum_ref[0:1, :] = jnp.sum(grad.T, axis=0, keepdims=True)
    sum_ref[1:2, :] = jnp.sum((grad * norm_ref[...]).T, axis=0, keepdims=True)


def shards(
    cotangent,
    mixer_out,
    expert_ids,
    route_weight,
    saved_normalized,
    inverse_deviation,
    channel_norm_gain,
    taps,
    proj_weight,
    gate_weight,
    up_weight,
    down_weight,
):
    sp = ("z", "x")
    experts = lax.axis_size(sp)
    ny = lax.axis_size("y")
    tok, width = cotangent.shape

    def flip_c(value):
        return lax.ppermute(value, "c", [(0, 1), (1, 0)])

    def hop(value, sign):
        pairs = []
        for y in range(ny):
            for c in range(2):
                pairs.append((2 * y + c, 2 * ((y + (sign if c == 0 else -sign)) % ny) + c))
        return lax.ppermute(value, ("y", "c"), pairs)

    own = kernel(
        pack_body, shape(3, width, 128), 1000000, gate_weight[0], up_weight[0], down_weight[0]
    )
    by_y = hop(own, 1)
    by_c = flip_c(own)
    by_yc = flip_c(by_y)

    rows = experts * 2 * SPAN
    ids, weights = expert_ids.T, route_weight.T
    sent = kernel(
        head_body, shape(rows, width), 2000000000, ids, weights, mixer_out, cotangent
    )
    got = lax.all_to_all(sent.reshape(experts, 2 * SPAN, width), sp, 0, 0, tiled=True)
    table = kernel(table_body, shape(2 * tok, experts * ny * 2 * SPAN), 2000000000, ids)

    normalized = saved_normalized.astype(F32)
    values = normalized * channel_norm_gain[None, :]
    gate = jax.nn.sigmoid(values)
    act_conv = (values * gate).astype(BF)
    slope = gate * (1.0 + values * (1.0 - gate)) * channel_norm_gain[None, :]

    slots = experts * SPAN
    x, g, hidden, back = kernel(
        expert_body,
        (shape(slots, width), shape(slots, width), shape(slots, 1536), shape(experts // 2, 128, 128)),
        4000000000,
        got.reshape(rows, width),
        own,
        by_c,
        by_y,
        by_yc,
        far=(1, 2, 3, 4),
        scratch=(
            pltpu.VMEM((width, 1024), BF),
            pltpu.VMEM((width // 128, 512, 128), BF),
            pltpu.SemaphoreType.DMA((4, 3)),
        ),
    )
    home = lax.all_to_all(
        back.reshape(experts * ny, 2 * SPAN, 128), ("z", "x", "y"), 0, 0, tiled=True
    ).reshape(-1, 128)

    packed = shape(2, 3, width, 128)
    keep, give = kernel(grads_body, (packed, packed), 8000000000, x, g, hidden)
    given = flip_c(give)
    passing = (keep[1].astype(F32) + given[1].astype(F32)).astype(BF)
    passed = hop(passing, -1)
    final = (keep[0].astype(F32) + given[0].astype(F32) + passed.astype(F32)).astype(BF)
    grad_down = final[2].reshape(-1, 128, 128).transpose(1, 0, 2).reshape(128, width)

    mine, other = kernel(
        combine_body,
        (shape(tok, 128, kind=F32), shape(tok, 128)),
        200000000,
        table,
        home,
        cotangent,
    )
    other = flip_c(other)
    mix = kernel(mix_body, shape(ny, tok, 128), 1000000, mine, other)
    mine_all = lax.all_to_all(mix, "y", 0, 0, tiled=True)
    other_all = flip_c(mine_all)

    proj, grad_norm, sums = kernel(
        final_body,
        (shape(width, 128), shape(tok, 128, kind=F32), shape(2, 128, kind=F32)),
        2000000000,
        mine_all,
        other_all,
        proj_weight,
        act_conv,
        slope,
        normalized,
    )
    proj = lax.all_to_all(proj.reshape(experts, -1, 128), sp, 0, 0, tiled=True)
    grad_proj = jnp.sum(proj.astype(F32), axis=0)

    sums = sums + flip_c(sums)
    for bit in (1, 2, 4):
        sums = sums + hop(sums, bit)
    mean = sums / (128 * 2 * ny)
    conv = inverse_deviation[:, None] * (
        grad_norm - mean[0][:, None] - normalized * mean[1][:, None]
    )
    reach = taps.shape[0] - 1
    beyond = lax.ppermute(conv[:reach], sp, [(i + 1, i) for i in range(experts - 1)])
    extended = jnp.concatenate([conv, beyond], axis=0)
    result = jnp.zeros_like(conv)
    for j in range(reach + 1):
        result = result + taps[j][None, :] * extended[j : j + tok]
    return (result.astype(BF), grad_proj, final[0][None], final[1][None], grad_down[None])


def solution(mesh):
    fine = Mesh(mesh.devices.reshape(8, 4, 8, 2), ("z", "x", "y", "c"))
    sp, tp = ("z", "x"), ("y", "c")
    return jax.shard_map(
        shards,
        mesh=fine,
        in_specs=(
            P(sp, None),
            P(sp, None),
            P(sp, None),
            P(sp, None),
            P(sp, tp),
            P(sp),
            P(tp),
            P(None, tp),
            P(tp, None),
            P(sp, None, tp),
            P(sp, None, tp),
            P(sp, tp, None),
        ),
        out_specs=(
            P(sp, tp),
            P(sp, tp),
            P(sp, None, tp),
            P(sp, None, tp),
            P(sp, tp, None),
        ),
        check_vma=False,
    )
```

```python
import jax
import jax.numpy as jnp
from jax import lax
from jax.experimental import pallas as pl
from jax.experimental.pallas import tpu as pltpu
from jax.sharding import Mesh, PartitionSpec as P


BF, F32, I32 = jnp.bfloat16, jnp.float32, jnp.int32
LAST = (((1,), (1,)), ((), ()))
FIRST = (((0,), (0,)), ((), ()))
SPAN = 4
VMEM = pl.BlockSpec(memory_space=pltpu.VMEM)
ANY = pl.BlockSpec(memory_space=pl.ANY)


def mm(a, b, dims=(((1,), (0,)), ((), ()))):
    return lax.dot_general(a, b, dims, preferred_element_type=F32)


def iota(shape, dim):
    return lax.broadcasted_iota(I32, shape, dim)


def kernel(body, outs, flops, *args, scratch=(), far=(), near=True):
    return pl.pallas_call(
        body,
        out_shape=outs,
        in_specs=[ANY if i in far else VMEM for i in range(len(args))],
        scratch_shapes=list(scratch),
        out_specs=jax.tree.map(lambda _: VMEM if near else ANY, outs),
        cost_estimate=pl.CostEstimate(flops=flops, bytes_accessed=1 << 20, transcendentals=0),
    )(*args)


def shape(*dims, kind=BF):
    return jax.ShapeDtypeStruct(dims, kind)


def head_body(ids_ref, weight_ref, mix_ref, cot_ref, out_ref):
    tok = ids_ref.shape[1]
    experts = out_ref.shape[0] // (2 * SPAN)
    group = (lax.axis_index("y") % 2) * 2 + lax.axis_index("c")
    ids = [ids_ref[k : k + 1, :] for k in range(2)]
    wts = [weight_ref[k : k + 1, :] for k in range(2)]
    expert = iota((experts, tok), 0)
    hot = [(expert == i).astype(F32) for i in ids]
    after = (iota((tok, tok), 0) < iota((tok, tok), 1)).astype(BF)
    rank = mm((hot[0] + hot[1]).astype(BF), after)
    rows = out_ref.shape[0]
    row = iota((rows, tok), 0)
    row_e, row_j = row // (2 * SPAN), row % (2 * SPAN)
    target = group * SPAN + row_j % SPAN
    found = jnp.zeros((rows, tok), jnp.bool_)
    scale = jnp.zeros((rows, tok), F32)
    for i, w, h in zip(ids, wts, hot):
        place = jnp.sum(rank * h, axis=0, keepdims=True).astype(I32)
        match = (row_e == i) & (target == place)
        found = found | match
        scale = jnp.where(match, w, scale)
    scale = jnp.sum(scale, axis=1, keepdims=True)
    is_x = row_j < SPAN
    take_x = jnp.where(found & is_x, 1.0, 0.0).astype(BF)
    take_g = jnp.where(found & ~is_x, 1.0, 0.0).astype(BF)
    scale = jnp.where(iota((rows, 1), 0) % (2 * SPAN) < SPAN, 1.0, scale)
    step = 512
    for at in range(0, mix_ref.shape[1], step):
        picked = mm(take_x, mix_ref[:, at : at + step]) + mm(take_g, cot_ref[:, at : at + step])
        out_ref[:, at : at + step] = (picked * scale).astype(BF)


def table_body(ids_ref, out_ref):
    tok = ids_ref.shape[1]
    ci = lax.axis_index("c")
    cols = out_ref.shape[1]
    experts = cols // 64
    lane = iota((tok, experts), 1)
    hot = jnp.zeros((tok, experts), F32)
    for k in range(2):
        ids = jnp.broadcast_to(ids_ref[k : k + 1, :].astype(F32), (tok, tok)).T
        hot = hot + (lane == ids[:, :experts].astype(I32)).astype(F32)
    before = (iota((tok, tok), 0) > iota((tok, tok), 1)).astype(BF)
    slot = jnp.where(hot > 0, mm(before, hot.astype(BF)), -1.0)
    spread = (iota((experts, cols), 1) // 64 == iota((experts, cols), 0)).astype(BF)
    held = mm(slot.astype(BF), spread).astype(I32)
    col = iota((tok, cols), 1)
    place = ((col // 8) % 2 * 2 + ci) * SPAN + col % SPAN
    half = (col // SPAN) % 2
    hit = held == place
    out_ref[:tok, :] = jnp.where(hit & (half == ci), 1.0, 0.0).astype(BF)
    out_ref[tok:, :] = jnp.where(hit & (half != ci), 1.0, 0.0).astype(BF)


def pack_body(gate_ref, up_ref, down_ref, out_ref, buf_ref, sem):
    blocks = down_ref.shape[1] // 128
    load, store = [], []
    for m, ref in enumerate((gate_ref, up_ref)):
        load.append(pltpu.make_async_copy(ref, buf_ref.at[m], sem.at[m, 0]))
    down = [
        pltpu.make_async_copy(
            down_ref.at[:, j * 128 : (j + 1) * 128],
            buf_ref.at[2, j * 128 : (j + 1) * 128],
            sem.at[2 + j, 0],
        )
        for j in range(blocks)
    ]
    for copy in (*load, *down):
        copy.start()
    for m in range(3):
        for copy in load[m : m + 1] if m < 2 else down:
            copy.wait()
        copy = pltpu.make_async_copy(buf_ref.at[m], out_ref.at[m], sem.at[m, 1])
        copy.start()
        store.append(copy)
    for copy in store:
        copy.wait()


def slope_body(saved_ref, gain_ref, proj_ref, act_ref, slope_ref, keep_ref, give_ref):
    ci = lax.axis_index("c")
    saved = saved_ref[...].astype(F32)
    values = saved * gain_ref[...]
    gate = jax.nn.sigmoid(values)
    act_ref[...] = (values * gate).astype(BF)
    slope = gate * (1.0 + values * (1.0 - gate)) * gain_ref[...]
    slope_ref[...] = slope
    high, low = [], []
    for u in (slope, slope * saved):
        high.append(u.astype(BF))
        low.append((u - high[-1].astype(F32)).astype(BF))
    high, low = jnp.concatenate(high, axis=0), jnp.concatenate(low, axis=0)
    for y in range(keep_ref.shape[0]):
        for ref, cc in ((keep_ref, ci), (give_ref, 1 - ci)):
            part = proj_ref[:, pl.ds(pl.multiple_of((2 * y + cc) * 128, 128), 128)]
            ref[y] = (mm(high, part) + mm(low, part)).astype(ref.dtype)


def share_body(keep_ref, given_ref, own_ref, *out_refs):
    yi = lax.axis_index("y")
    ny = keep_ref.shape[0]
    own_ref[...] = keep_ref[yi] + given_ref[yi].astype(F32)
    for k, ref in enumerate(out_refs, 1):
        to = lax.rem(yi + k, ny)
        ref[...] = (keep_ref[to] + given_ref[to].astype(F32)).astype(BF)


def total_body(own_ref, *refs):
    total = own_ref[...]
    for ref in refs[:-1]:
        total = total + ref[...].astype(F32)
    refs[-1][...] = total


def expert_body(got_ref, w0, w1, w2, w3, x_ref, g_ref, hid_ref, back_ref, in_ref, down_ref, sem):
    rows, width = got_ref.shape
    slots = rows // 2
    copies = []
    for q, w in enumerate((w0, w1, w2, w3)):
        three = []
        for m in range(2):
            at = (2 * q + m) * 128
            three.append(pltpu.make_async_copy(w.at[m], in_ref.at[:, at : at + 128], sem.at[q, m]))
        down = w.at[2].reshape(width // 128, 128, 128)
        three.append(
            pltpu.make_async_copy(down, down_ref.at[:, q * 128 : (q + 1) * 128, :], sem.at[q, 2])
        )
        for copy in three:
            copy.start()
        copies.append(three)
    out_row, in_row = iota((slots, rows), 0), iota((slots, rows), 1)
    want = (out_row // SPAN) * (2 * SPAN) + out_row % SPAN
    pick_x = (in_row == want).astype(BF)
    pick_g = (in_row == want + SPAN).astype(BF)
    for at in range(0, width, 512):
        part = got_ref[:, at : at + 512]
        x_ref[:, at : at + 512] = mm(pick_x, part).astype(BF)
        g_ref[:, at : at + 512] = mm(pick_g, part).astype(BF)
    for q in range(4):
        for copy in copies[q]:
            copy.wait()
        both = mm(x_ref[...], in_ref[:, q * 256 : (q + 1) * 256])
        hg, hu = both[:, :128], both[:, 128:]
        gact = jnp.zeros((slots, 128), F32)
        for j in range(0, width // 128, 2):
            blocks = [down_ref[j + i, q * 128 : (q + 1) * 128, :] for i in range(2)]
            gact = gact + mm(
                g_ref[:, j * 128 : (j + 2) * 128], jnp.concatenate(blocks, axis=1), LAST
            )
        sigma = jax.nn.sigmoid(hg)
        swish = hg * sigma
        at = q * 256
        hid_ref[:, at : at + 128] = (gact * hu * sigma * (1.0 + hg * (1.0 - sigma))).astype(BF)
        hid_ref[:, at + 128 : at + 256] = (gact * swish).astype(BF)
        hid_ref[:, 1024 + q * 128 : 1152 + q * 128] = (swish * hu).astype(BF)
    low = iota((slots, 128), 0) % (2 * SPAN) < SPAN
    for y in range(width // 256):
        both = mm(hid_ref[:, :1024], in_ref[y * 256 : (y + 1) * 256, :], LAST)
        pair = [both[:, :128], both[:, 128:]]
        even = jnp.where(low, pair[0], pltpu.roll(pair[1], SPAN, 0))
        odd = jnp.where(low, pltpu.roll(pair[0], slots - SPAN, 0), pair[1])
        back_ref[:, y * 8 : (y + 1) * 8, :] = even.reshape(-1, 8, 128).astype(BF)
        back_ref[:, 64 + y * 8 : 64 + (y + 1) * 8, :] = odd.reshape(-1, 8, 128).astype(BF)


def grads_body(x_ref, g_ref, hid_ref, keep_ref, give_ref):
    width = x_ref.shape[1]
    places = ((keep_ref, 0), (give_ref, 0), (keep_ref, 1), (give_ref, 1))
    for j in range(width // 128):
        at = slice(j * 128, (j + 1) * 128)
        both = mm(x_ref[:, at], hid_ref[:, :1024], FIRST)
        down = mm(hid_ref[:, 1024:], g_ref[:, at], FIRST)
        for q, (ref, to) in enumerate(places):
            ref[to, 0, at, :] = both[:, q * 256 : q * 256 + 128].astype(BF)
            ref[to, 1, at, :] = both[:, q * 256 + 128 : (q + 1) * 256].astype(BF)
            ref[to, 2, at, :] = down[q * 128 : (q + 1) * 128, :].astype(BF)


def combine_body(table_ref, home_ref, cot_ref, own_ref, other_ref):
    tok = cot_ref.shape[0]
    place = lax.axis_index("y") * 2 + lax.axis_index("c")
    cot = cot_ref[:, pl.ds(pl.multiple_of(place * 128, 128), 128)].astype(F32)
    both = mm(table_ref[...], home_ref[...])
    own_ref[...] = both[:tok] + cot
    other_ref[...] = both[tok:].astype(BF)


def mix_body(own_ref, other_ref, total_ref, out_ref):
    tok = own_ref.shape[0]
    mix = (own_ref[...] + other_ref[...].astype(F32)).astype(BF)
    wide = mix.astype(F32)
    parts = []
    for k in range(2):
        rest = jnp.sum((wide * total_ref[k * tok : (k + 1) * tok, :]).T, axis=0, keepdims=True)
        for _ in range(3):
            parts.append(rest.astype(BF).astype(F32))
            rest = rest - parts[-1]
    parts.append(jnp.zeros((2, tok), F32))
    sums = jnp.concatenate(parts, axis=0).astype(BF)
    for y in range(out_ref.shape[0]):
        out_ref[y, :tok, :] = mix
        out_ref[y, tok:, :] = sums


def final_body(mine_ref, other_ref, proj_ref, act_ref, slope_ref, saved_ref, dev_ref, out_ref, conv_ref):
    ci = lax.axis_index("c")
    tok = act_ref.shape[0]
    acc = jnp.zeros((tok, tok), F32)
    sums = jnp.zeros((8, tok), F32)
    for y in range(mine_ref.shape[0]):
        for ref, cc in ((mine_ref, ci), (other_ref, 1 - ci)):
            at = pl.ds(pl.multiple_of((2 * y + cc) * 128, 128), 128)
            part = ref[y, :tok, :]
            sums = sums + ref[y, tok:, :].astype(F32)
            out_ref[at, :] = mm(part, act_ref[...], FIRST).astype(BF)
            acc = acc + mm(part, proj_ref[:, at], LAST)
    grad = acc * slope_ref[...]
    count = 2 * mine_ref.shape[0] * 128
    means = []
    for k in range(2):
        total = jnp.sum(sums[3 * k : 3 * k + 3], axis=0, keepdims=True) / count
        means.append(jnp.broadcast_to(total, (tok, tok)).T)
    dev = jnp.broadcast_to(dev_ref[...], (tok, tok)).T
    conv_ref[...] = dev * (grad - means[0] - saved_ref[...].astype(F32) * means[1])


def sumout_body(keep_ref, given_ref, pre_ref, pass_ref):
    pre_ref[0] = (keep_ref[0, 0].astype(F32) + given_ref[0, 0].astype(F32)).astype(BF)
    pass_ref[0] = (keep_ref[1, 0].astype(F32) + given_ref[1, 0].astype(F32)).astype(BF)


def addup_body(pre_ref, passed_ref, gate_ref, up_ref, down_ref):
    for m, ref in ((0, gate_ref), (1, up_ref)):
        ref[...] = (pre_ref[m].astype(F32) + passed_ref[m].astype(F32)).astype(BF)
    for j in range(down_ref.shape[1] // 128):
        at = slice(j * 128, (j + 1) * 128)
        down_ref[:, at] = (pre_ref[2, at].astype(F32) + passed_ref[2, at].astype(F32)).astype(BF)


def shards(
    cotangent,
    mixer_out,
    expert_ids,
    route_weight,
    saved_normalized,
    inverse_deviation,
    channel_norm_gain,
    taps,
    proj_weight,
    gate_weight,
    up_weight,
    down_weight,
):
    sp = ("z", "x")
    experts = lax.axis_size(sp)
    ny = lax.axis_size("y")
    tok, width = cotangent.shape

    def flip_c(value):
        return lax.ppermute(value, "c", [(0, 1), (1, 0)])

    def shift(value, k):
        return lax.ppermute(value, "y", [(i, (i + k) % ny) for i in range(ny)])

    def hop(value, sign):
        pairs = []
        for y in range(ny):
            for c in range(2):
                pairs.append((2 * y + c, 2 * ((y + (sign if c == 0 else -sign)) % ny) + c))
        return lax.ppermute(value, ("y", "c"), pairs)

    own = kernel(
        pack_body,
        shape(3, width, 128),
        1000000,
        gate_weight[0],
        up_weight[0],
        down_weight[0],
        far=(0, 1, 2),
        near=False,
        scratch=(pltpu.VMEM((3, width, 128), BF), pltpu.SemaphoreType.DMA((2 + width // 128, 2))),
    )
    by_y = hop(own, 1)
    by_c = flip_c(own)
    by_yc = flip_c(by_y)

    rows = experts * 2 * SPAN
    ids, weights = expert_ids.T, route_weight.T
    sent = kernel(
        head_body, shape(rows, width), 2000000000, ids, weights, mixer_out, cotangent
    )
    got = lax.all_to_all(sent.reshape(experts, 2 * SPAN, width), sp, 0, 0, tiled=True)
    table = kernel(table_body, shape(2 * tok, experts * ny * 2 * SPAN), 2000000000, ids)

    act_conv, slope, vkeep, vgive = kernel(
        slope_body,
        (
            shape(tok, 128),
            shape(tok, 128, kind=F32),
            shape(ny, 2 * tok, 128, kind=F32),
            shape(ny, 2 * tok, 128),
        ),
        500000000,
        saved_normalized,
        channel_norm_gain[None, :],
        proj_weight,
    )
    vgiven = flip_c(vgive)
    vown, *vsent = kernel(
        share_body,
        (shape(2 * tok, 128, kind=F32), *[shape(2 * tok, 128)] * (ny - 1)),
        1000000,
        vkeep,
        vgiven,
    )
    vgot = []
    for k, value in enumerate(vsent, 1):
        vgot.append(shift(value, k))
    vtotal = kernel(total_body, shape(2 * tok, 128, kind=F32), 1000000, vown, *vgot)

    slots = experts * SPAN
    x, g, hidden, back = kernel(
        expert_body,
        (shape(slots, width), shape(slots, width), shape(slots, 1536), shape(experts // 2, 128, 128)),
        4000000000,
        got.reshape(rows, width),
        own,
        by_c,
        by_y,
        by_yc,
        far=(1, 2, 3, 4),
        scratch=(
            pltpu.VMEM((width, 1024), BF),
            pltpu.VMEM((width // 128, 512, 128), BF),
            pltpu.SemaphoreType.DMA((4, 3)),
        ),
    )
    home = lax.all_to_all(
        back.reshape(experts * ny, 2 * SPAN, 128), ("z", "x", "y"), 0, 0, tiled=True
    ).reshape(-1, 128)

    packed = shape(2, 3, width, 128)
    keep, give = kernel(grads_body, (packed, packed), 8000000000, x, g, hidden)
    given = flip_c(give)
    block = pl.BlockSpec((2, 1, width, 128), lambda m: (0, m, 0, 0))
    piece = pl.BlockSpec((1, width, 128), lambda m: (m, 0, 0))
    before, passing = pl.pallas_call(
        sumout_body,
        grid=(3,),
        out_shape=(shape(3, width, 128), shape(3, width, 128)),
        in_specs=[block, block],
        out_specs=[piece, piece],
        cost_estimate=pl.CostEstimate(flops=1000000, bytes_accessed=9 << 20, transcendentals=0),
    )(keep, given)
    passed = hop(passing, -1)
    grad_gate, grad_up, grad_down = kernel(
        addup_body,
        (shape(width, 128), shape(width, 128), shape(128, width)),
        1000000,
        before,
        passed,
    )

    mine, other = kernel(
        combine_body,
        (shape(tok, 128, kind=F32), shape(tok, 128)),
        200000000,
        table,
        home,
        cotangent,
    )
    other = flip_c(other)
    mix = kernel(mix_body, shape(ny, tok + 8, 128), 1000000, mine, other, vtotal)
    mine_all = lax.all_to_all(mix, "y", 0, 0, tiled=True)
    other_all = flip_c(mine_all)

    proj, conv = kernel(
        final_body,
        (shape(width, 128), shape(tok, 128, kind=F32)),
        2000000000,
        mine_all,
        other_all,
        proj_weight,
        act_conv,
        slope,
        saved_normalized,
        inverse_deviation[None, :],
    )
    proj = lax.all_to_all(proj.reshape(experts, -1, 128), sp, 0, 0, tiled=True)
    grad_proj = jnp.sum(proj.astype(F32), axis=0)

    reach = taps.shape[0] - 1
    beyond = lax.ppermute(conv[:reach], sp, [(i + 1, i) for i in range(experts - 1)])
    extended = jnp.concatenate([conv, beyond], axis=0)
    result = jnp.zeros_like(conv)
    for j in range(reach + 1):
        result = result + taps[j][None, :] * extended[j : j + tok]
    return (result.astype(BF), grad_proj, grad_gate[None], grad_up[None], grad_down[None])


def solution(mesh):
    fine = Mesh(mesh.devices.reshape(8, 4, 8, 2), ("z", "x", "y", "c"))
    sp, tp = ("z", "x"), ("y", "c")
    return jax.shard_map(
        shards,
        mesh=fine,
        in_specs=(
            P(sp, None),
            P(sp, None),
            P(sp, None),
            P(sp, None),
            P(sp, tp),
            P(sp),
            P(tp),
            P(None, tp),
            P(tp, None),
            P(sp, None, tp),
            P(sp, None, tp),
            P(sp, tp, None),
        ),
        out_specs=(
            P(sp, tp),
            P(sp, tp),
            P(sp, None, tp),
            P(sp, None, tp),
            P(sp, tp, None),
        ),
        check_vma=False,
    )
```

```python
import functools

import jax
import jax.numpy as jnp
from jax import lax
from jax.experimental import pallas as pl
from jax.experimental.pallas import tpu as pltpu
from jax.sharding import Mesh, PartitionSpec as P


BF, F32, I32 = jnp.bfloat16, jnp.float32, jnp.int32
LAST = (((1,), (1,)), ((), ()))
FIRST = (((0,), (0,)), ((), ()))
SPAN = 4
VMEM = pl.BlockSpec(memory_space=pltpu.VMEM)
ANY = pl.BlockSpec(memory_space=pl.ANY)


def mm(a, b, dims=(((1,), (0,)), ((), ()))):
    return lax.dot_general(a, b, dims, preferred_element_type=F32)


def iota(shape, dim):
    return lax.broadcasted_iota(I32, shape, dim)


def kernel(body, outs, flops, *args, scratch=(), far=(), far_out=()):
    many = outs if isinstance(outs, tuple) else (outs,)
    specs = [ANY if i in far_out else VMEM for i in range(len(many))]
    return pl.pallas_call(
        body,
        out_shape=outs,
        in_specs=[ANY if i in far else VMEM for i in range(len(args))],
        out_specs=specs if isinstance(outs, tuple) else specs[0],
        scratch_shapes=list(scratch),
        cost_estimate=pl.CostEstimate(flops=flops, bytes_accessed=1 << 20, transcendentals=0),
    )(*args)


def shape(*dims, kind=BF):
    return jax.ShapeDtypeStruct(dims, kind)


def head_body(
    ids_ref, weight_ref, mix_ref, cot_ref, gate_ref, up_ref, down_ref, out_ref, pack_ref, buf_ref, sem
):
    load = []
    for m, ref in enumerate((gate_ref, up_ref)):
        load.append([pltpu.make_async_copy(ref, buf_ref.at[m], sem.at[m, 0])])
    down = []
    for j in range(down_ref.shape[1] // 128):
        at = slice(j * 128, (j + 1) * 128)
        down.append(
            pltpu.make_async_copy(down_ref.at[:, at], buf_ref.at[2, at], sem.at[2 + j, 0])
        )
    load.append(down)
    for copies in load:
        for copy in copies:
            copy.start()
    tok = ids_ref.shape[1]
    experts = out_ref.shape[0] // (2 * SPAN)
    group = (lax.axis_index("y") % 2) * 2 + lax.axis_index("c")
    ids = [ids_ref[k : k + 1, :] for k in range(2)]
    wts = [weight_ref[k : k + 1, :] for k in range(2)]
    expert = iota((experts, tok), 0)
    hot = [(expert == i).astype(F32) for i in ids]
    after = (iota((tok, tok), 0) < iota((tok, tok), 1)).astype(BF)
    rank = mm((hot[0] + hot[1]).astype(BF), after)
    rows = out_ref.shape[0]
    row = iota((rows, tok), 0)
    row_e, row_j = row // (2 * SPAN), row % (2 * SPAN)
    target = group * SPAN + row_j % SPAN
    found = jnp.zeros((rows, tok), jnp.bool_)
    scale = jnp.zeros((rows, tok), F32)
    for i, w, h in zip(ids, wts, hot):
        place = jnp.sum(rank * h, axis=0, keepdims=True).astype(I32)
        match = (row_e == i) & (target == place)
        found = found | match
        scale = jnp.where(match, w, scale)
    scale = jnp.sum(scale, axis=1, keepdims=True)
    is_x = row_j < SPAN
    take_x = jnp.where(found & is_x, 1.0, 0.0).astype(BF)
    take_g = jnp.where(found & ~is_x, 1.0, 0.0).astype(BF)
    scale = jnp.where(iota((rows, 1), 0) % (2 * SPAN) < SPAN, 1.0, scale)
    store = []
    for m, copies in enumerate(load):
        for copy in copies:
            copy.wait()
        store.append(pltpu.make_async_copy(buf_ref.at[m], pack_ref.at[m], sem.at[m, 1]))
        store[-1].start()
    step = 512
    for at in range(0, mix_ref.shape[1], step):
        picked = mm(take_x, mix_ref[:, at : at + step]) + mm(take_g, cot_ref[:, at : at + step])
        out_ref[:, at : at + step] = (picked * scale).astype(BF)
    for copy in store:
        copy.wait()


def table_body(ids_ref, out_ref):
    tok = ids_ref.shape[1]
    ci = lax.axis_index("c")
    cols = out_ref.shape[1]
    experts = cols // 64
    lane = iota((tok, experts), 1)
    hot = jnp.zeros((tok, experts), F32)
    for k in range(2):
        ids = jnp.broadcast_to(ids_ref[k : k + 1, :].astype(F32), (tok, tok)).T
        hot = hot + (lane == ids[:, :experts].astype(I32)).astype(F32)
    before = (iota((tok, tok), 0) > iota((tok, tok), 1)).astype(BF)
    slot = jnp.where(hot > 0, mm(before, hot.astype(BF)), -1.0)
    spread = (iota((experts, cols), 1) // 64 == iota((experts, cols), 0)).astype(BF)
    held = mm(slot.astype(BF), spread).astype(I32)
    col = iota((tok, cols), 1)
    place = ((col // 8) % 2 * 2 + ci) * SPAN + col % SPAN
    half = (col // SPAN) % 2
    hit = held == place
    out_ref[:tok, :] = jnp.where(hit & (half == ci), 1.0, 0.0).astype(BF)
    out_ref[tok:, :] = jnp.where(hit & (half != ci), 1.0, 0.0).astype(BF)


def slope_body(saved_ref, gain_ref, proj_ref, act_ref, slope_ref, keep_ref, give_ref):
    ci = lax.axis_index("c")
    saved = saved_ref[...].astype(F32)
    values = saved * gain_ref[...]
    gate = jax.nn.sigmoid(values)
    act_ref[...] = (values * gate).astype(BF)
    slope = gate * (1.0 + values * (1.0 - gate)) * gain_ref[...]
    slope_ref[...] = slope
    high, low = [], []
    for u in (slope, slope * saved):
        high.append(u.astype(BF))
        low.append((u - high[-1].astype(F32)).astype(BF))
    high, low = jnp.concatenate(high, axis=0), jnp.concatenate(low, axis=0)
    for y in range(keep_ref.shape[0]):
        for ref, cc in ((keep_ref, ci), (give_ref, 1 - ci)):
            part = proj_ref[:, pl.ds(pl.multiple_of((2 * y + cc) * 128, 128), 128)]
            ref[y] = (mm(high, part) + mm(low, part)).astype(ref.dtype)


def share_body(bit, keep_ref, given_ref, own_ref, send_ref):
    side = lax.rem(lax.axis_index("y") // (1 << bit), 2)
    for i in range(keep_ref.shape[0] // 2):
        for ref, at in ((own_ref, 2 * i + side), (send_ref, 2 * i + 1 - side)):
            ref[i] = (keep_ref[at] + given_ref[at].astype(F32)).astype(ref.dtype)


def expert_body(got_ref, w0, w1, w2, w3, x_ref, g_ref, hid_ref, back_ref, in_ref, down_ref, sem):
    rows, width = got_ref.shape
    slots = rows // 2
    copies = []
    for q, w in enumerate((w0, w1, w2, w3)):
        three = []
        for m in range(2):
            at = (2 * q + m) * 128
            three.append(pltpu.make_async_copy(w.at[m], in_ref.at[:, at : at + 128], sem.at[q, m]))
        down = w.at[2].reshape(width // 128, 128, 128)
        three.append(
            pltpu.make_async_copy(down, down_ref.at[:, q * 128 : (q + 1) * 128, :], sem.at[q, 2])
        )
        for copy in three:
            copy.start()
        copies.append(three)
    out_row, in_row = iota((slots, rows), 0), iota((slots, rows), 1)
    want = (out_row // SPAN) * (2 * SPAN) + out_row % SPAN
    pick_x = (in_row == want).astype(BF)
    pick_g = (in_row == want + SPAN).astype(BF)
    for at in range(0, width, 512):
        part = got_ref[:, at : at + 512]
        x_ref[:, at : at + 512] = mm(pick_x, part).astype(BF)
        g_ref[:, at : at + 512] = mm(pick_g, part).astype(BF)
    for q in range(4):
        for copy in copies[q]:
            copy.wait()
        both = mm(x_ref[...], in_ref[:, q * 256 : (q + 1) * 256])
        hg, hu = both[:, :128], both[:, 128:]
        gact = jnp.zeros((slots, 128), F32)
        for j in range(0, width // 128, 2):
            blocks = [down_ref[j + i, q * 128 : (q + 1) * 128, :] for i in range(2)]
            gact = gact + mm(
                g_ref[:, j * 128 : (j + 2) * 128], jnp.concatenate(blocks, axis=1), LAST
            )
        sigma = jax.nn.sigmoid(hg)
        swish = hg * sigma
        at = q * 256
        hid_ref[:, at : at + 128] = (gact * hu * sigma * (1.0 + hg * (1.0 - sigma))).astype(BF)
        hid_ref[:, at + 128 : at + 256] = (gact * swish).astype(BF)
        hid_ref[:, 1024 + q * 128 : 1152 + q * 128] = (swish * hu).astype(BF)
    low = iota((slots, 128), 0) % (2 * SPAN) < SPAN
    for y in range(width // 256):
        both = mm(hid_ref[:, :1024], in_ref[y * 256 : (y + 1) * 256, :], LAST)
        pair = [both[:, :128], both[:, 128:]]
        even = jnp.where(low, pair[0], pltpu.roll(pair[1], SPAN, 0))
        odd = jnp.where(low, pltpu.roll(pair[0], slots - SPAN, 0), pair[1])
        back_ref[:, y * 8 : (y + 1) * 8, :] = even.reshape(-1, 8, 128).astype(BF)
        back_ref[:, 64 + y * 8 : 64 + (y + 1) * 8, :] = odd.reshape(-1, 8, 128).astype(BF)


def grads_body(x_ref, g_ref, hid_ref, keep_ref, give_ref):
    width = x_ref.shape[1]
    places = ((keep_ref, 0), (give_ref, 0), (keep_ref, 1), (give_ref, 1))
    for j in range(width // 128):
        at = slice(j * 128, (j + 1) * 128)
        both = mm(x_ref[:, at], hid_ref[:, :1024], FIRST)
        down = mm(hid_ref[:, 1024:], g_ref[:, at], FIRST)
        for q, (ref, to) in enumerate(places):
            ref[to, 0, at, :] = both[:, q * 256 : q * 256 + 128].astype(BF)
            ref[to, 1, at, :] = both[:, q * 256 + 128 : (q + 1) * 256].astype(BF)
            ref[to, 2, at, :] = down[q * 128 : (q + 1) * 128, :].astype(BF)


def combine_body(table_ref, home_ref, cot_ref, own_ref, other_ref):
    tok = cot_ref.shape[0]
    place = lax.axis_index("y") * 2 + lax.axis_index("c")
    cot = cot_ref[:, pl.ds(pl.multiple_of(place * 128, 128), 128)].astype(F32)
    both = mm(table_ref[...], home_ref[...])
    own_ref[...] = both[:tok] + cot
    other_ref[...] = both[tok:].astype(BF)


def mix_body(own_ref, other_ref, vown_ref, vgot_ref, out_ref):
    tok = own_ref.shape[0]
    total = vown_ref[0] + vgot_ref[0].astype(F32)
    mix = (own_ref[...] + other_ref[...].astype(F32)).astype(BF)
    wide = mix.astype(F32)
    parts = []
    for k in range(2):
        rest = jnp.sum((wide * total[k * tok : (k + 1) * tok, :]).T, axis=0, keepdims=True)
        for _ in range(3):
            parts.append(rest.astype(BF).astype(F32))
            rest = rest - parts[-1]
    parts.append(jnp.zeros((2, tok), F32))
    sums = jnp.concatenate(parts, axis=0).astype(BF)
    for y in range(out_ref.shape[0]):
        out_ref[y, :tok, :] = mix
        out_ref[y, tok:, :] = sums


def final_body(all_ref, proj_ref, act_ref, slope_ref, saved_ref, dev_ref, out_ref, conv_ref):
    tok = act_ref.shape[0]
    acc = jnp.zeros((tok, tok), F32)
    sums = jnp.zeros((8, tok), F32)
    for t in range(all_ref.shape[0]):
        at = slice(t * 128, (t + 1) * 128)
        part = all_ref[t, :tok, :]
        sums = sums + all_ref[t, tok:, :].astype(F32)
        out_ref[at, :] = mm(part, act_ref[...], FIRST).astype(BF)
        acc = acc + mm(part, proj_ref[:, at], LAST)
    grad = acc * slope_ref[...]
    count = all_ref.shape[0] * 128
    means = []
    for k in range(2):
        total = jnp.sum(sums[3 * k : 3 * k + 3], axis=0, keepdims=True) / count
        means.append(jnp.broadcast_to(total, (tok, tok)).T)
    dev = jnp.broadcast_to(dev_ref[...], (tok, tok)).T
    conv_ref[...] = dev * (grad - means[0] - saved_ref[...].astype(F32) * means[1])


def sumout_body(keep_ref, given_ref, pre_ref, pass_ref):
    pre_ref[0] = (keep_ref[0, 0].astype(F32) + given_ref[0, 0].astype(F32)).astype(BF)
    pass_ref[0] = (keep_ref[1, 0].astype(F32) + given_ref[1, 0].astype(F32)).astype(BF)


def addup_body(pre_ref, passed_ref, gate_ref, up_ref, down_ref):
    for m, ref in ((0, gate_ref), (1, up_ref)):
        ref[...] = (pre_ref[m].astype(F32) + passed_ref[m].astype(F32)).astype(BF)
    for j in range(down_ref.shape[1] // 128):
        at = slice(j * 128, (j + 1) * 128)
        down_ref[:, at] = (pre_ref[2, at].astype(F32) + passed_ref[2, at].astype(F32)).astype(BF)


def shards(
    cotangent,
    mixer_out,
    expert_ids,
    route_weight,
    saved_normalized,
    inverse_deviation,
    channel_norm_gain,
    taps,
    proj_weight,
    gate_weight,
    up_weight,
    down_weight,
):
    sp = ("z", "x")
    experts = lax.axis_size(sp)
    ny = lax.axis_size("y")
    tok, width = cotangent.shape

    def flip_c(value):
        return lax.ppermute(value, "c", [(0, 1), (1, 0)])

    def flip_y(value, bit):
        return lax.ppermute(value, "y", [(i, i ^ (1 << bit)) for i in range(ny)])

    def hop(value, sign):
        pairs = []
        for y in range(ny):
            for c in range(2):
                pairs.append((2 * y + c, 2 * ((y + (sign if c == 0 else -sign)) % ny) + c))
        return lax.ppermute(value, ("y", "c"), pairs)

    rows = experts * 2 * SPAN
    ids, weights = expert_ids.T, route_weight.T
    sent, own = kernel(
        head_body,
        (shape(rows, width), shape(3, width, 128)),
        2000000000,
        ids,
        weights,
        mixer_out,
        cotangent,
        gate_weight[0],
        up_weight[0],
        down_weight[0],
        far=(4, 5, 6),
        far_out=(1,),
        scratch=(pltpu.VMEM((3, width, 128), BF), pltpu.SemaphoreType.DMA((2 + width // 128, 2))),
    )
    by_y = hop(own, 1)
    by_c = flip_c(own)
    by_yc = flip_c(by_y)

    got = lax.all_to_all(sent.reshape(experts, 2 * SPAN, width), sp, 0, 0, tiled=True)
    table = kernel(table_body, shape(2 * tok, experts * ny * 2 * SPAN), 2000000000, ids)

    act_conv, slope, vkeep, vgive = kernel(
        slope_body,
        (
            shape(tok, 128),
            shape(tok, 128, kind=F32),
            shape(ny, 2 * tok, 128, kind=F32),
            shape(ny, 2 * tok, 128),
        ),
        500000000,
        saved_normalized,
        channel_norm_gain[None, :],
        proj_weight,
    )
    vgiven = flip_c(vgive)
    for bit in range(3):
        half = ny >> (bit + 1)
        vkeep, vgive = kernel(
            functools.partial(share_body, bit),
            (shape(half, 2 * tok, 128, kind=F32), shape(half, 2 * tok, 128)),
            1000000,
            vkeep,
            vgiven,
        )
        vgiven = flip_y(vgive, bit)

    slots = experts * SPAN
    x, g, hidden, back = kernel(
        expert_body,
        (shape(slots, width), shape(slots, width), shape(slots, 1536), shape(experts // 2, 128, 128)),
        4000000000,
        got.reshape(rows, width),
        own,
        by_c,
        by_y,
        by_yc,
        far=(1, 2, 3, 4),
        scratch=(
            pltpu.VMEM((width, 1024), BF),
            pltpu.VMEM((width // 128, 512, 128), BF),
            pltpu.SemaphoreType.DMA((4, 3)),
        ),
    )
    home = lax.all_to_all(
        back.reshape(experts * ny, 2 * SPAN, 128), ("z", "x", "y"), 0, 0, tiled=True
    ).reshape(-1, 128)

    packed = shape(2, 3, width, 128)
    keep, give = kernel(grads_body, (packed, packed), 8000000000, x, g, hidden)
    given = flip_c(give)
    block = pl.BlockSpec((2, 1, width, 128), lambda m: (0, m, 0, 0))
    piece = pl.BlockSpec((1, width, 128), lambda m: (m, 0, 0))
    before, passing = pl.pallas_call(
        sumout_body,
        grid=(3,),
        out_shape=(shape(3, width, 128), shape(3, width, 128)),
        in_specs=[block, block],
        out_specs=[piece, piece],
        cost_estimate=pl.CostEstimate(flops=1000000, bytes_accessed=9 << 20, transcendentals=0),
    )(keep, given)
    passed = hop(passing, -1)
    grad_gate, grad_up, grad_down = kernel(
        addup_body,
        (shape(width, 128), shape(width, 128), shape(128, width)),
        1000000,
        before,
        passed,
    )

    mine, other = kernel(
        combine_body,
        (shape(tok, 128, kind=F32), shape(tok, 128)),
        200000000,
        table,
        home,
        cotangent,
    )
    other = flip_c(other)
    mix = kernel(
        mix_body, shape(2 * ny, tok + 8, 128), 1000000, mine, other, vkeep, vgiven
    )
    mix_all = lax.all_to_all(mix, ("y", "c"), 0, 0, tiled=True)

    proj, conv = kernel(
        final_body,
        (shape(width, 128), shape(tok, 128, kind=F32)),
        2000000000,
        mix_all,
        proj_weight,
        act_conv,
        slope,
        saved_normalized,
        inverse_deviation[None, :],
    )
    proj = lax.all_to_all(proj.reshape(experts, -1, 128), sp, 0, 0, tiled=True)
    grad_proj = jnp.sum(proj.astype(F32), axis=0)

    reach = taps.shape[0] - 1
    beyond = lax.ppermute(conv[:reach], sp, [(i + 1, i) for i in range(experts - 1)])
    extended = jnp.concatenate([conv, beyond], axis=0)
    result = jnp.zeros_like(conv)
    for j in range(reach + 1):
        result = result + taps[j][None, :] * extended[j : j + tok]
    return (result.astype(BF), grad_proj, grad_gate[None], grad_up[None], grad_down[None])


def solution(mesh):
    fine = Mesh(mesh.devices.reshape(8, 4, 8, 2), ("z", "x", "y", "c"))
    sp, tp = ("z", "x"), ("y", "c")
    return jax.shard_map(
        shards,
        mesh=fine,
        in_specs=(
            P(sp, None),
            P(sp, None),
            P(sp, None),
            P(sp, None),
            P(sp, tp),
            P(sp),
            P(tp),
            P(None, tp),
            P(tp, None),
            P(sp, None, tp),
            P(sp, None, tp),
            P(sp, tp, None),
        ),
        out_specs=(
            P(sp, tp),
            P(sp, tp),
            P(sp, None, tp),
            P(sp, None, tp),
            P(sp, tp, None),
        ),
        check_vma=False,
    )
```

```python
import functools

import jax
import jax.numpy as jnp
from jax import lax
from jax.experimental import pallas as pl
from jax.experimental.pallas import tpu as pltpu
from jax.sharding import Mesh, PartitionSpec as P


BF, F32, I32 = jnp.bfloat16, jnp.float32, jnp.int32
LAST = (((1,), (1,)), ((), ()))
FIRST = (((0,), (0,)), ((), ()))
SPAN = 4
VMEM = pl.BlockSpec(memory_space=pltpu.VMEM)
ANY = pl.BlockSpec(memory_space=pl.ANY)
HBM = pl.BlockSpec(memory_space=pltpu.HBM)


def mm(a, b, dims=(((1,), (0,)), ((), ()))):
    return lax.dot_general(a, b, dims, preferred_element_type=F32)


def iota(shape, dim):
    return lax.broadcasted_iota(I32, shape, dim)


def kernel(body, outs, flops, *args, scratch=(), any_in=(), far=(), far_out=(), limit=60 * 1024):
    many = outs if isinstance(outs, tuple) else (outs,)
    specs = [HBM if i in far_out else VMEM for i in range(len(many))]
    return pl.pallas_call(
        body,
        out_shape=outs,
        in_specs=[
            HBM if i in far else ANY if i in any_in else VMEM for i in range(len(args))
        ],
        out_specs=specs if isinstance(outs, tuple) else specs[0],
        scratch_shapes=list(scratch),
        compiler_params=pltpu.CompilerParams(vmem_limit_bytes=limit << 10),
        cost_estimate=pl.CostEstimate(flops=flops, bytes_accessed=1 << 20, transcendentals=0),
    )(*args)


def shape(*dims, kind=BF):
    return jax.ShapeDtypeStruct(dims, kind)


def head_body(
    ids_ref,
    weight_ref,
    mix_any,
    cot_any,
    gate_ref,
    up_ref,
    down_ref,
    out_any,
    pack_ref,
    mix_ref,
    cot_ref,
    out_ref,
    buf_ref,
    in_sem,
    out_sem,
):
    tokens = [
        pltpu.make_async_copy(mix_any, mix_ref, in_sem.at[0]),
        pltpu.make_async_copy(cot_any, cot_ref, in_sem.at[1]),
    ]
    load = []
    for m, ref in enumerate((gate_ref, up_ref)):
        load.append([pltpu.make_async_copy(ref, buf_ref.at[m], in_sem.at[2 + m])])
    down = []
    for j in range(down_ref.shape[1] // 128):
        at = slice(j * 128, (j + 1) * 128)
        down.append(pltpu.make_async_copy(down_ref.at[:, at], buf_ref.at[2, at], in_sem.at[4 + j]))
    load.append(down)
    for copies in (tokens, *load):
        for copy in copies:
            copy.start()
    tok = ids_ref.shape[1]
    rows = out_ref.shape[0]
    experts = rows // (2 * SPAN)
    group = (lax.axis_index("y") % 2) * 2 + lax.axis_index("c")
    ids = [ids_ref[k : k + 1, :] for k in range(2)]
    wts = [weight_ref[k : k + 1, :] for k in range(2)]
    expert = iota((experts, tok), 0)
    hot = [(expert == i).astype(F32) for i in ids]
    after = (iota((tok, tok), 0) < iota((tok, tok), 1)).astype(BF)
    rank = mm((hot[0] + hot[1]).astype(BF), after)
    row = iota((rows, tok), 0)
    row_e, row_j = row // (2 * SPAN), row % (2 * SPAN)
    target = group * SPAN + row_j % SPAN
    found = jnp.zeros((rows, tok), jnp.bool_)
    scale = jnp.zeros((rows, tok), F32)
    for i, w, h in zip(ids, wts, hot):
        place = jnp.sum(rank * h, axis=0, keepdims=True).astype(I32)
        match = (row_e == i) & (target == place)
        found = found | match
        scale = jnp.where(match, w, scale)
    scale = jnp.sum(scale, axis=1, keepdims=True)
    is_x = row_j < SPAN
    take_x = jnp.where(found & is_x, 1.0, 0.0).astype(BF)
    take_g = jnp.where(found & ~is_x, 1.0, 0.0).astype(BF)
    scale = jnp.where(iota((rows, 1), 0) % (2 * SPAN) < SPAN, 1.0, scale)
    for copy in tokens:
        copy.wait()
    store = []
    for m, copies in enumerate(load):
        for copy in copies:
            copy.wait()
        store.append(pltpu.make_async_copy(buf_ref.at[m], pack_ref.at[m], out_sem.at[m]))
        store[-1].start()
    step = 512
    for k, at in enumerate(range(0, mix_ref.shape[1], step)):
        cut = slice(at, at + step)
        picked = mm(take_x, mix_ref[:, cut]) + mm(take_g, cot_ref[:, cut])
        out_ref[:, cut] = (picked * scale).astype(BF)
        store.append(
            pltpu.make_async_copy(out_ref.at[:, cut], out_any.at[:, cut], out_sem.at[3 + k])
        )
        store[-1].start()
    for copy in store:
        copy.wait()


def table_body(ids_ref, out_ref):
    tok = ids_ref.shape[1]
    ci = lax.axis_index("c")
    cols = out_ref.shape[1]
    experts = cols // 16
    lane = iota((tok, experts), 1)
    hot = jnp.zeros((tok, experts), F32)
    for k in range(2):
        ids = jnp.broadcast_to(ids_ref[k : k + 1, :].astype(F32), (tok, tok)).T
        hot = hot + (lane == ids[:, :experts].astype(I32)).astype(F32)
    before = (iota((tok, tok), 0) > iota((tok, tok), 1)).astype(BF)
    slot = jnp.where(hot > 0, mm(before, hot.astype(BF)), -1.0)
    spread = (iota((experts, cols), 1) // 16 == iota((experts, cols), 0)).astype(BF)
    held = mm(slot.astype(BF), spread).astype(I32)
    col = iota((tok, cols), 1)
    place = ((col // 8) % 2 * 2 + ci) * SPAN + col % SPAN
    half = (col // SPAN) % 2
    hit = held == place
    out_ref[:tok, :] = jnp.where(hit & (half == ci), 1.0, 0.0).astype(BF)
    out_ref[tok:, :] = jnp.where(hit & (half != ci), 1.0, 0.0).astype(BF)


def slope_body(saved_ref, gain_ref, proj_ref, act_ref, slope_ref, keep_ref, give_ref):
    ci = lax.axis_index("c")
    saved = saved_ref[...].astype(F32)
    values = saved * gain_ref[...]
    gate = jax.nn.sigmoid(values)
    act_ref[...] = (values * gate).astype(BF)
    slope = gate * (1.0 + values * (1.0 - gate)) * gain_ref[...]
    slope_ref[...] = slope
    high, low = [], []
    for u in (slope, slope * saved):
        high.append(u.astype(BF))
        low.append((u - high[-1].astype(F32)).astype(BF))
    high, low = jnp.concatenate(high, axis=0), jnp.concatenate(low, axis=0)
    for y in range(keep_ref.shape[0]):
        for ref, cc in ((keep_ref, ci), (give_ref, 1 - ci)):
            part = proj_ref[:, pl.ds(pl.multiple_of((2 * y + cc) * 128, 128), 128)]
            ref[y] = (mm(high, part) + mm(low, part)).astype(ref.dtype)


def share_body(bit, keep_ref, given_ref, own_ref, send_ref):
    side = lax.rem(lax.axis_index("y") // (1 << bit), 2)
    for i in range(keep_ref.shape[0] // 2):
        for ref, at in ((own_ref, 2 * i + side), (send_ref, 2 * i + 1 - side)):
            ref[i] = (keep_ref[at] + given_ref[at].astype(F32)).astype(ref.dtype)


def pickers(slots):
    out_row, in_row = iota((slots, 2 * slots), 0), iota((slots, 2 * slots), 1)
    want = (out_row // SPAN) * (2 * SPAN) + out_row % SPAN
    return (in_row == want).astype(BF), (in_row == want + SPAN).astype(BF)


def expert_body(got_ref, w0, w1, w2, w3, hid_ref, back_ref, x_ref, g_ref, in_ref, down_ref, sem):
    rows, width = got_ref.shape
    slots = rows // 2
    copies = []
    for q, w in enumerate((w0, w1, w2, w3)):
        three = []
        for m in range(2):
            at = (2 * q + m) * 128
            three.append(pltpu.make_async_copy(w.at[m], in_ref.at[:, at : at + 128], sem.at[q, m]))
        down = w.at[2].reshape(width // 128, 128, 128)
        three.append(
            pltpu.make_async_copy(down, down_ref.at[:, q * 128 : (q + 1) * 128, :], sem.at[q, 2])
        )
        for copy in three:
            copy.start()
        copies.append(three)
    pick_x, pick_g = pickers(slots)
    for at in range(0, width, 512):
        part = got_ref[:, at : at + 512]
        x_ref[:, at : at + 512] = mm(pick_x, part).astype(BF)
        g_ref[:, at : at + 512] = mm(pick_g, part).astype(BF)
    for q in range(4):
        for copy in copies[q]:
            copy.wait()
        both = mm(x_ref[...], in_ref[:, q * 256 : (q + 1) * 256])
        hg, hu = both[:, :128], both[:, 128:]
        gact = jnp.zeros((slots, 128), F32)
        for j in range(0, width // 128, 2):
            blocks = [down_ref[j + i, q * 128 : (q + 1) * 128, :] for i in range(2)]
            gact = gact + mm(
                g_ref[:, j * 128 : (j + 2) * 128], jnp.concatenate(blocks, axis=1), LAST
            )
        sigma = jax.nn.sigmoid(hg)
        swish = hg * sigma
        at = q * 256
        hid_ref[:, at : at + 128] = (gact * hu * sigma * (1.0 + hg * (1.0 - sigma))).astype(BF)
        hid_ref[:, at + 128 : at + 256] = (gact * swish).astype(BF)
        hid_ref[:, 1024 + q * 128 : 1152 + q * 128] = (swish * hu).astype(BF)
    low = iota((slots, 128), 0) % (2 * SPAN) < SPAN
    for y in range(width // 256):
        both = mm(hid_ref[:, :1024], in_ref[y * 256 : (y + 1) * 256, :], LAST)
        pair = [both[:, :128], both[:, 128:]]
        even = jnp.where(low, pair[0], pltpu.roll(pair[1], SPAN, 0))
        odd = jnp.where(low, pltpu.roll(pair[0], slots - SPAN, 0), pair[1])
        back_ref[:, y * 8 : (y + 1) * 8, :] = even.reshape(-1, 8, 128).astype(BF)
        back_ref[:, 64 + y * 8 : 64 + (y + 1) * 8, :] = odd.reshape(-1, 8, 128).astype(BF)


def grads_body(got_ref, hid_ref, keep_ref, give_ref):
    pick_x, pick_g = pickers(got_ref.shape[0] // 2)
    places = ((keep_ref, 0), (give_ref, 0), (keep_ref, 1), (give_ref, 1))
    for j in range(got_ref.shape[1] // 128):
        at = slice(j * 128, (j + 1) * 128)
        both = mm(mm(pick_x, got_ref[:, at]).astype(BF), hid_ref[:, :1024], FIRST)
        down = mm(hid_ref[:, 1024:], mm(pick_g, got_ref[:, at]).astype(BF), FIRST)
        for q, (ref, to) in enumerate(places):
            ref[to, 0, at, :] = both[:, q * 256 : q * 256 + 128].astype(BF)
            ref[to, 1, at, :] = both[:, q * 256 + 128 : (q + 1) * 256].astype(BF)
            ref[to, 2, at, :] = down[q * 128 : (q + 1) * 128, :].astype(BF)


def combine_body(table_ref, home_ref, cot_any, own_ref, other_ref, cot_ref, sem):
    tok = cot_ref.shape[0]
    place = lax.axis_index("y") * 2 + lax.axis_index("c")
    cut = pl.ds(pl.multiple_of(place * 128, 128), 128)
    copy = pltpu.make_async_copy(cot_any.at[:, cut], cot_ref, sem)
    copy.start()
    cols = table_ref.shape[1]
    part = home_ref[...].astype(F32).reshape(cols // 16, -1, 16, 128)
    total = part[:, 0]
    for j in range(1, part.shape[1]):
        total = total + part[:, j]
    both = mm(table_ref[...], total.reshape(cols, 128).astype(BF))
    other_ref[...] = both[tok:].astype(BF)
    copy.wait()
    own_ref[...] = both[:tok] + cot_ref[...].astype(F32)


def mix_body(own_ref, other_ref, vown_ref, vgot_ref, out_ref, buf_ref, sem):
    tok = own_ref.shape[0]
    total = vown_ref[0] + vgot_ref[0].astype(F32)
    mix = (own_ref[...] + other_ref[...].astype(F32)).astype(BF)
    wide = mix.astype(F32)
    parts = []
    for k in range(2):
        rest = jnp.sum((wide * total[k * tok : (k + 1) * tok, :]).T, axis=0, keepdims=True)
        for _ in range(3):
            parts.append(rest.astype(BF).astype(F32))
            rest = rest - parts[-1]
    parts.append(jnp.zeros((2, tok), F32))
    sums = jnp.concatenate(parts, axis=0).astype(BF)
    buf_ref[:tok, :] = mix
    buf_ref[tok:, :] = sums
    copies = [
        pltpu.make_async_copy(buf_ref, out_ref.at[t], sem.at[t]) for t in range(out_ref.shape[0])
    ]
    for copy in copies:
        copy.start()
    for copy in copies:
        copy.wait()


def final_body(
    all_ref, proj_ref, act_ref, slope_ref, saved_ref, dev_ref, out_any, conv_ref, out_ref, sem
):
    tok = act_ref.shape[0]
    acc = jnp.zeros((tok, tok), F32)
    sums = jnp.zeros((8, tok), F32)
    copies = []
    for t in range(all_ref.shape[0]):
        at = slice(t * 128, (t + 1) * 128)
        out_ref[at, :] = mm(all_ref[t, :tok, :], act_ref[...], FIRST).astype(BF)
        if t % 4 == 3:
            at = slice((t - 3) * 128, (t + 1) * 128)
            copies.append(
                pltpu.make_async_copy(out_ref.at[at, :], out_any.at[at, :], sem.at[t // 4])
            )
            copies[-1].start()
    for t in range(0, all_ref.shape[0], 2):
        pair = [all_ref[t + i, :tok, :] for i in range(2)]
        acc = acc + mm(
            jnp.concatenate(pair, axis=1), proj_ref[:, t * 128 : (t + 2) * 128], LAST
        )
        for i in range(2):
            sums = sums + all_ref[t + i, tok:, :].astype(F32)
    grad = acc * slope_ref[...]
    count = all_ref.shape[0] * 128
    means = []
    for k in range(2):
        total = jnp.sum(sums[3 * k : 3 * k + 3], axis=0, keepdims=True) / count
        means.append(jnp.broadcast_to(total, (tok, tok)).T)
    dev = jnp.broadcast_to(dev_ref[...], (tok, tok)).T
    conv_ref[...] = dev * (grad - means[0] - saved_ref[...].astype(F32) * means[1])
    for copy in copies:
        copy.wait()


def sumout_body(keep_ref, given_ref, pre_ref, pass_ref):
    pre_ref[0] = (keep_ref[0, 0].astype(F32) + given_ref[0, 0].astype(F32)).astype(BF)
    pass_ref[0] = (keep_ref[1, 0].astype(F32) + given_ref[1, 0].astype(F32)).astype(BF)


def addup_body(pre_ref, passed_ref, gate_ref, up_ref, down_ref):
    for m, ref in ((0, gate_ref), (1, up_ref)):
        ref[...] = (pre_ref[m].astype(F32) + passed_ref[m].astype(F32)).astype(BF)
    for j in range(down_ref.shape[1] // 128):
        at = slice(j * 128, (j + 1) * 128)
        down_ref[:, at] = (pre_ref[2, at].astype(F32) + passed_ref[2, at].astype(F32)).astype(BF)


def shards(
    cotangent,
    mixer_out,
    expert_ids,
    route_weight,
    saved_normalized,
    inverse_deviation,
    channel_norm_gain,
    taps,
    proj_weight,
    gate_weight,
    up_weight,
    down_weight,
):
    sp = ("z", "x")
    experts = lax.axis_size(sp)
    ny = lax.axis_size("y")
    tok, width = cotangent.shape

    def flip_c(value):
        return lax.ppermute(value, "c", [(0, 1), (1, 0)])

    def flip_y(value, bit):
        return lax.ppermute(value, "y", [(i, i ^ (1 << bit)) for i in range(ny)])

    def hop(value, sign):
        pairs = []
        for y in range(ny):
            for c in range(2):
                pairs.append((2 * y + c, 2 * ((y + (sign if c == 0 else -sign)) % ny) + c))
        return lax.ppermute(value, ("y", "c"), pairs)

    rows = experts * 2 * SPAN
    ids, weights = expert_ids.T, route_weight.T
    sent, own = kernel(
        head_body,
        (shape(rows, width), shape(3, width, 128)),
        2000000000,
        ids,
        weights,
        mixer_out,
        cotangent,
        gate_weight[0],
        up_weight[0],
        down_weight[0],
        far=(2, 3, 4, 5, 6),
        far_out=(0, 1),
        scratch=(
            pltpu.VMEM((tok, width), BF),
            pltpu.VMEM((tok, width), BF),
            pltpu.VMEM((rows, width), BF),
            pltpu.VMEM((3, width, 128), BF),
            pltpu.SemaphoreType.DMA((4 + width // 128,)),
            pltpu.SemaphoreType.DMA((3 + width // 512,)),
        ),
    )
    by_y = hop(own, 1)
    by_c = flip_c(own)
    by_yc = flip_c(by_y)

    got = lax.all_to_all(sent.reshape(experts, 2 * SPAN, width), sp, 0, 0, tiled=True)
    table = kernel(table_body, shape(2 * tok, experts * 4 * SPAN), 500000000, ids, limit=12 << 10)

    act_conv, slope, vkeep, vgive = kernel(
        slope_body,
        (
            shape(tok, 128),
            shape(tok, 128, kind=F32),
            shape(ny, 2 * tok, 128, kind=F32),
            shape(ny, 2 * tok, 128),
        ),
        500000000,
        saved_normalized,
        channel_norm_gain[None, :],
        proj_weight,
        limit=16 << 10,
    )
    vgiven = flip_c(vgive)
    for bit in range(3):
        half = ny >> (bit + 1)
        vkeep, vgive = kernel(
            functools.partial(share_body, bit),
            (shape(half, 2 * tok, 128, kind=F32), shape(half, 2 * tok, 128)),
            1000000,
            vkeep,
            vgiven,
            limit=12 << 10,
        )
        vgiven = flip_y(vgive, bit)

    slots = experts * SPAN
    got = got.reshape(rows, width)
    hidden, back = kernel(
        expert_body,
        (shape(slots, 1536), shape(experts // 2, 128, 128)),
        4000000000,
        got,
        own,
        by_c,
        by_y,
        by_yc,
        any_in=(1, 2, 3, 4),
        limit=24 << 10,
        scratch=(
            pltpu.VMEM((slots, width), BF),
            pltpu.VMEM((slots, width), BF),
            pltpu.VMEM((width, 1024), BF),
            pltpu.VMEM((width // 128, 512, 128), BF),
            pltpu.SemaphoreType.DMA((4, 3)),
        ),
    )
    home = lax.all_to_all(
        back.reshape(experts * ny, 2 * SPAN, 128), ("z", "x", "y"), 0, 0, tiled=True
    ).reshape(-1, 128)

    packed = shape(2, 3, width, 128)
    quarter = pl.BlockSpec((2, 3, width // 4, 128), lambda j: (0, 0, j, 0))
    keep, give = pl.pallas_call(
        grads_body,
        grid=(4,),
        out_shape=(packed, packed),
        in_specs=[
            pl.BlockSpec((rows, width // 4), lambda j: (0, j)),
            pl.BlockSpec((slots, 1536), lambda j: (0, 0)),
        ],
        out_specs=[quarter, quarter],
        cost_estimate=pl.CostEstimate(flops=8000000000, bytes_accessed=7 << 20, transcendentals=0),
    )(got, hidden)
    given = flip_c(give)
    block = pl.BlockSpec((2, 1, width, 128), lambda m: (0, m, 0, 0))
    piece = pl.BlockSpec((1, width, 128), lambda m: (m, 0, 0))
    before, passing = pl.pallas_call(
        sumout_body,
        grid=(3,),
        out_shape=(shape(3, width, 128), shape(3, width, 128)),
        in_specs=[block, block],
        out_specs=[piece, piece],
        cost_estimate=pl.CostEstimate(flops=1000000, bytes_accessed=9 << 20, transcendentals=0),
    )(keep, given)
    passed = hop(passing, -1)
    grad_gate, grad_up, grad_down = kernel(
        addup_body,
        (shape(width, 128), shape(width, 128), shape(128, width)),
        1000000,
        before,
        passed,
        limit=20 << 10,
    )

    mine, other = kernel(
        combine_body,
        (shape(tok, 128, kind=F32), shape(tok, 128)),
        200000000,
        table,
        home,
        cotangent,
        far=(2,),
        limit=12 << 10,
        scratch=(pltpu.VMEM((tok, 128), BF), pltpu.SemaphoreType.DMA),
    )
    other = flip_c(other)
    mix = kernel(
        mix_body,
        shape(2 * ny, tok + 8, 128),
        1000000,
        mine,
        other,
        vkeep,
        vgiven,
        far_out=(0,),
        limit=12 << 10,
        scratch=(pltpu.VMEM((tok + 8, 128), BF), pltpu.SemaphoreType.DMA((2 * ny,))),
    )
    mix_all = lax.all_to_all(mix, ("y", "c"), 0, 0, tiled=True)

    proj, conv = kernel(
        final_body,
        (shape(width, 128), shape(tok, 128, kind=F32)),
        2000000000,
        mix_all,
        proj_weight,
        act_conv,
        slope,
        saved_normalized,
        inverse_deviation[None, :],
        far_out=(0,),
        limit=16 << 10,
        scratch=(pltpu.VMEM((width, 128), BF), pltpu.SemaphoreType.DMA((ny // 2,))),
    )
    proj = lax.all_to_all(proj.reshape(experts, -1, 128), sp, 0, 0, tiled=True)
    grad_proj = jnp.sum(proj.astype(F32), axis=0)

    reach = taps.shape[0] - 1
    beyond = lax.ppermute(conv[:reach], sp, [(i + 1, i) for i in range(experts - 1)])
    extended = jnp.concatenate([conv, beyond], axis=0)
    result = jnp.zeros_like(conv)
    for j in range(reach + 1):
        result = result + taps[j][None, :] * extended[j : j + tok]
    return (result.astype(BF), grad_proj, grad_gate[None], grad_up[None], grad_down[None])


def solution(mesh):
    fine = Mesh(mesh.devices.reshape(8, 4, 8, 2), ("z", "x", "y", "c"))
    sp, tp = ("z", "x"), ("y", "c")
    return jax.shard_map(
        shards,
        mesh=fine,
        in_specs=(
            P(sp, None),
            P(sp, None),
            P(sp, None),
            P(sp, None),
            P(sp, tp),
            P(sp),
            P(tp),
            P(None, tp),
            P(tp, None),
            P(sp, None, tp),
            P(sp, None, tp),
            P(sp, tp, None),
        ),
        out_specs=(
            P(sp, tp),
            P(sp, tp),
            P(sp, None, tp),
            P(sp, None, tp),
            P(sp, tp, None),
        ),
        check_vma=False,
    )
```

```python
import functools

import jax
import jax.numpy as jnp
from jax import lax
from jax.experimental import pallas as pl
from jax.experimental.pallas import tpu as pltpu
from jax.sharding import Mesh, PartitionSpec as P


BF, F32, I32 = jnp.bfloat16, jnp.float32, jnp.int32
LAST = (((1,), (1,)), ((), ()))
FIRST = (((0,), (0,)), ((), ()))
SPAN = 4
VMEM = pl.BlockSpec(memory_space=pltpu.VMEM)
HBM = pl.BlockSpec(memory_space=pltpu.HBM)


def mm(a, b, dims=(((1,), (0,)), ((), ()))):
    return lax.dot_general(a, b, dims, preferred_element_type=F32)


def iota(shape, dim):
    return lax.broadcasted_iota(I32, shape, dim)


def kernel(body, outs, flops, *args, scratch=(), far=(), far_out=(), limit=60 * 1024):
    many = outs if isinstance(outs, tuple) else (outs,)
    specs = [HBM if i in far_out else VMEM for i in range(len(many))]
    return pl.pallas_call(
        body,
        out_shape=outs,
        in_specs=[
            HBM if i in far else VMEM for i in range(len(args))
        ],
        out_specs=specs if isinstance(outs, tuple) else specs[0],
        scratch_shapes=list(scratch),
        compiler_params=pltpu.CompilerParams(vmem_limit_bytes=limit << 10),
        cost_estimate=pl.CostEstimate(flops=flops, bytes_accessed=1 << 20, transcendentals=0),
    )(*args)


def shape(*dims, kind=BF):
    return jax.ShapeDtypeStruct(dims, kind)


def head_body(
    ids_ref,
    weight_ref,
    mix_any,
    cot_any,
    gate_ref,
    up_ref,
    down_ref,
    out_any,
    pack_ref,
    mix_ref,
    cot_ref,
    out_ref,
    buf_ref,
    in_sem,
    out_sem,
):
    tokens = [
        pltpu.make_async_copy(mix_any, mix_ref, in_sem.at[0]),
        pltpu.make_async_copy(cot_any, cot_ref, in_sem.at[1]),
    ]
    load = []
    for m, ref in enumerate((gate_ref, up_ref)):
        load.append([pltpu.make_async_copy(ref, buf_ref.at[m], in_sem.at[2 + m])])
    down = []
    for j in range(down_ref.shape[1] // 128):
        at = slice(j * 128, (j + 1) * 128)
        down.append(pltpu.make_async_copy(down_ref.at[:, at], buf_ref.at[2, at], in_sem.at[4 + j]))
    load.append(down)
    for copies in (tokens, *load):
        for copy in copies:
            copy.start()
    tok = ids_ref.shape[1]
    rows = out_ref.shape[0]
    experts = rows // (2 * SPAN)
    group = (lax.axis_index("y") % 2) * 2 + lax.axis_index("c")
    ids = [ids_ref[k : k + 1, :] for k in range(2)]
    wts = [weight_ref[k : k + 1, :] for k in range(2)]
    expert = iota((experts, tok), 0)
    hot = [(expert == i).astype(F32) for i in ids]
    after = (iota((tok, tok), 0) < iota((tok, tok), 1)).astype(BF)
    rank = mm((hot[0] + hot[1]).astype(BF), after)
    row = iota((rows, tok), 0)
    row_e, row_j = row // (2 * SPAN), row % (2 * SPAN)
    target = group * SPAN + row_j % SPAN
    found = jnp.zeros((rows, tok), jnp.bool_)
    scale = jnp.zeros((rows, tok), F32)
    for i, w, h in zip(ids, wts, hot):
        place = jnp.sum(rank * h, axis=0, keepdims=True).astype(I32)
        match = (row_e == i) & (target == place)
        found = found | match
        scale = jnp.where(match, w, scale)
    scale = jnp.sum(scale, axis=1, keepdims=True)
    is_x = row_j < SPAN
    take_x = jnp.where(found & is_x, 1.0, 0.0).astype(BF)
    take_g = jnp.where(found & ~is_x, 1.0, 0.0).astype(BF)
    scale = jnp.where(iota((rows, 1), 0) % (2 * SPAN) < SPAN, 1.0, scale)
    for copy in tokens:
        copy.wait()
    store = []
    for m, copies in enumerate(load):
        for copy in copies:
            copy.wait()
        store.append(pltpu.make_async_copy(buf_ref.at[m], pack_ref.at[m], out_sem.at[m]))
        store[-1].start()
    step = 512
    for k, at in enumerate(range(0, mix_ref.shape[1], step)):
        cut = slice(at, at + step)
        picked = mm(take_x, mix_ref[:, cut]) + mm(take_g, cot_ref[:, cut])
        out_ref[:, cut] = (picked * scale).astype(BF)
        store.append(
            pltpu.make_async_copy(out_ref.at[:, cut], out_any.at[:, cut], out_sem.at[3 + k])
        )
        store[-1].start()
    for copy in store:
        copy.wait()


def table_body(ids_ref, out_ref):
    tok = ids_ref.shape[1]
    ci = lax.axis_index("c")
    cols = out_ref.shape[1]
    experts = cols // 16
    lane = iota((tok, experts), 1)
    hot = jnp.zeros((tok, experts), F32)
    for k in range(2):
        ids = jnp.broadcast_to(ids_ref[k : k + 1, :].astype(F32), (tok, tok)).T
        hot = hot + (lane == ids[:, :experts].astype(I32)).astype(F32)
    before = (iota((tok, tok), 0) > iota((tok, tok), 1)).astype(BF)
    slot = jnp.where(hot > 0, mm(before, hot.astype(BF)), -1.0)
    spread = (iota((experts, cols), 1) // 16 == iota((experts, cols), 0)).astype(BF)
    held = mm(slot.astype(BF), spread).astype(I32)
    col = iota((tok, cols), 1)
    place = ((col // 8) % 2 * 2 + ci) * SPAN + col % SPAN
    half = (col // SPAN) % 2
    hit = held == place
    out_ref[:tok, :] = jnp.where(hit & (half == ci), 1.0, 0.0).astype(BF)
    out_ref[tok:, :] = jnp.where(hit & (half != ci), 1.0, 0.0).astype(BF)


def slope_body(saved_ref, gain_ref, proj_ref, act_ref, slope_ref, keep_ref, give_ref):
    ci = lax.axis_index("c")
    saved = saved_ref[...].astype(F32)
    values = saved * gain_ref[...]
    gate = jax.nn.sigmoid(values)
    act_ref[...] = (values * gate).astype(BF)
    slope = gate * (1.0 + values * (1.0 - gate)) * gain_ref[...]
    slope_ref[...] = slope
    high, low = [], []
    for u in (slope, slope * saved):
        high.append(u.astype(BF))
        low.append((u - high[-1].astype(F32)).astype(BF))
    high, low = jnp.concatenate(high, axis=0), jnp.concatenate(low, axis=0)
    for y in range(keep_ref.shape[0]):
        for ref, cc in ((keep_ref, ci), (give_ref, 1 - ci)):
            part = proj_ref[:, pl.ds(pl.multiple_of((2 * y + cc) * 128, 128), 128)]
            ref[y] = (mm(high, part) + mm(low, part)).astype(ref.dtype)


def share_body(bit, keep_ref, given_ref, own_ref, send_ref):
    side = lax.rem(lax.axis_index("y") // (1 << bit), 2)
    for i in range(keep_ref.shape[0] // 2):
        for ref, at in ((own_ref, 2 * i + side), (send_ref, 2 * i + 1 - side)):
            ref[i] = (keep_ref[at] + given_ref[at].astype(F32)).astype(ref.dtype)


def pickers(slots):
    out_row, in_row = iota((slots, 2 * slots), 0), iota((slots, 2 * slots), 1)
    want = (out_row // SPAN) * (2 * SPAN) + out_row % SPAN
    return (in_row == want).astype(BF), (in_row == want + SPAN).astype(BF)


def expert_body(got_ref, w0, w1, w2, w3, hid_ref, back_ref, x_ref, g_ref, in_ref, down_ref, sem):
    rows, width = got_ref.shape
    slots = rows // 2
    copies = []
    for q, w in enumerate((w0, w1, w2, w3)):
        three = []
        for m in range(2):
            at = (2 * q + m) * 128
            three.append(pltpu.make_async_copy(w.at[m], in_ref.at[:, at : at + 128], sem.at[q, m]))
        down = w.at[2].reshape(width // 128, 128, 128)
        three.append(
            pltpu.make_async_copy(down, down_ref.at[:, q * 128 : (q + 1) * 128, :], sem.at[q, 2])
        )
        for copy in three:
            copy.start()
        copies.append(three)
    pick_x, pick_g = pickers(slots)
    for at in range(0, width, 512):
        part = got_ref[:, at : at + 512]
        x_ref[:, at : at + 512] = mm(pick_x, part).astype(BF)
        g_ref[:, at : at + 512] = mm(pick_g, part).astype(BF)
    for q in range(4):
        for copy in copies[q]:
            copy.wait()
        both = mm(x_ref[...], in_ref[:, q * 256 : (q + 1) * 256])
        hg, hu = both[:, :128], both[:, 128:]
        gact = jnp.zeros((slots, 128), F32)
        for j in range(0, width // 128, 2):
            blocks = [down_ref[j + i, q * 128 : (q + 1) * 128, :] for i in range(2)]
            gact = gact + mm(
                g_ref[:, j * 128 : (j + 2) * 128], jnp.concatenate(blocks, axis=1), LAST
            )
        sigma = jax.nn.sigmoid(hg)
        swish = hg * sigma
        at = q * 256
        hid_ref[:, at : at + 128] = (gact * hu * sigma * (1.0 + hg * (1.0 - sigma))).astype(BF)
        hid_ref[:, at + 128 : at + 256] = (gact * swish).astype(BF)
        hid_ref[:, 1024 + q * 128 : 1152 + q * 128] = (swish * hu).astype(BF)
    low = iota((slots, 128), 0) % (2 * SPAN) < SPAN
    for y in range(width // 256):
        both = mm(hid_ref[:, :1024], in_ref[y * 256 : (y + 1) * 256, :], LAST)
        pair = [both[:, :128], both[:, 128:]]
        even = jnp.where(low, pair[0], pltpu.roll(pair[1], SPAN, 0))
        odd = jnp.where(low, pltpu.roll(pair[0], slots - SPAN, 0), pair[1])
        back_ref[:, y * 8 : (y + 1) * 8, :] = even.reshape(-1, 8, 128).astype(BF)
        back_ref[:, 64 + y * 8 : 64 + (y + 1) * 8, :] = odd.reshape(-1, 8, 128).astype(BF)


def grads_body(got_ref, hid_ref, keep_ref, give_ref):
    pick_x, pick_g = pickers(got_ref.shape[0] // 2)
    places = ((keep_ref, 0), (give_ref, 0), (keep_ref, 1), (give_ref, 1))
    x = mm(pick_x, got_ref[...]).astype(BF)
    g = mm(pick_g, got_ref[...]).astype(BF)
    for q, (ref, to) in enumerate(places):
        both = mm(x, hid_ref[:, q * 256 : (q + 1) * 256], FIRST)
        ref[to, 0] = both[:, :128].astype(BF)
        ref[to, 1] = both[:, 128:].astype(BF)
        down = mm(hid_ref[:, 1024 + q * 128 : 1152 + q * 128], g, FIRST)
        for j in range(got_ref.shape[1] // 128):
            at = slice(j * 128, (j + 1) * 128)
            ref[to, 2, at, :] = down[:, at].astype(BF)


def combine_body(table_ref, home_ref, cot_any, own_ref, other_ref, cot_ref, sem):
    tok = cot_ref.shape[0]
    place = lax.axis_index("y") * 2 + lax.axis_index("c")
    cut = pl.ds(pl.multiple_of(place * 128, 128), 128)
    copy = pltpu.make_async_copy(cot_any.at[:, cut], cot_ref, sem)
    copy.start()
    cols = table_ref.shape[1]
    part = home_ref[...].astype(F32).reshape(cols // 16, -1, 16, 128)
    total = part[:, 0]
    for j in range(1, part.shape[1]):
        total = total + part[:, j]
    both = mm(table_ref[...], total.reshape(cols, 128).astype(BF))
    other_ref[...] = both[tok:].astype(BF)
    copy.wait()
    own_ref[...] = both[:tok] + cot_ref[...].astype(F32)


def mix_body(own_ref, other_ref, vown_ref, vgot_ref, out_ref, buf_ref, sem):
    tok = own_ref.shape[0]
    total = vown_ref[0] + vgot_ref[0].astype(F32)
    mix = (own_ref[...] + other_ref[...].astype(F32)).astype(BF)
    wide = mix.astype(F32)
    parts = []
    for k in range(2):
        rest = jnp.sum((wide * total[k * tok : (k + 1) * tok, :]).T, axis=0, keepdims=True)
        for _ in range(3):
            parts.append(rest.astype(BF).astype(F32))
            rest = rest - parts[-1]
    parts.append(jnp.zeros((2, tok), F32))
    sums = jnp.concatenate(parts, axis=0).astype(BF)
    buf_ref[:tok, :] = mix
    buf_ref[tok:, :] = sums
    copies = [
        pltpu.make_async_copy(buf_ref, out_ref.at[t], sem.at[t]) for t in range(out_ref.shape[0])
    ]
    for copy in copies:
        copy.start()
    for copy in copies:
        copy.wait()


def proj_body(all_ref, act_ref, out_any, out_ref, sem):
    copies = []
    tok = act_ref.shape[0]
    for t in range(all_ref.shape[0]):
        at = slice(t * 128, (t + 1) * 128)
        out_ref[at, :] = mm(all_ref[t, :tok, :], act_ref[...], FIRST).astype(BF)
        if t % 4 == 3:
            at = slice((t - 3) * 128, (t + 1) * 128)
            copies.append(
                pltpu.make_async_copy(out_ref.at[at, :], out_any.at[at, :], sem.at[t // 4])
            )
            copies[-1].start()
    for copy in copies:
        copy.wait()


def norm_body(all_ref, proj_ref, slope_ref, saved_ref, dev_ref, conv_ref):
    tok = slope_ref.shape[0]
    acc = jnp.zeros((tok, tok), F32)
    sums = jnp.zeros((8, tok), F32)
    for t in range(0, all_ref.shape[0], 2):
        pair = [all_ref[t + i, :tok, :] for i in range(2)]
        acc = acc + mm(
            jnp.concatenate(pair, axis=1), proj_ref[:, t * 128 : (t + 2) * 128], LAST
        )
        for i in range(2):
            sums = sums + all_ref[t + i, tok:, :].astype(F32)
    grad = acc * slope_ref[...]
    count = all_ref.shape[0] * 128
    means = []
    for k in range(2):
        total = jnp.sum(sums[3 * k : 3 * k + 3], axis=0, keepdims=True) / count
        means.append(jnp.broadcast_to(total, (tok, tok)).T)
    dev = jnp.broadcast_to(dev_ref[...], (tok, tok)).T
    conv_ref[...] = dev * (grad - means[0] - saved_ref[...].astype(F32) * means[1])


def reduce_body(parts_ref, out_ref):
    out_ref[...] = jnp.sum(parts_ref[...].astype(F32), axis=0)


def sumout_body(keep_ref, given_ref, pre_ref, pass_ref):
    pre_ref[0] = (keep_ref[0, 0].astype(F32) + given_ref[0, 0].astype(F32)).astype(BF)
    pass_ref[0] = (keep_ref[1, 0].astype(F32) + given_ref[1, 0].astype(F32)).astype(BF)


def addup_body(pre_ref, passed_ref, gate_ref, up_ref, down_ref):
    for m, ref in ((0, gate_ref), (1, up_ref)):
        ref[...] = (pre_ref[m].astype(F32) + passed_ref[m].astype(F32)).astype(BF)
    for j in range(down_ref.shape[1] // 128):
        at = slice(j * 128, (j + 1) * 128)
        down_ref[:, at] = (pre_ref[2, at].astype(F32) + passed_ref[2, at].astype(F32)).astype(BF)


def shards(
    cotangent,
    mixer_out,
    expert_ids,
    route_weight,
    saved_normalized,
    inverse_deviation,
    channel_norm_gain,
    taps,
    proj_weight,
    gate_weight,
    up_weight,
    down_weight,
):
    sp = ("z", "x")
    experts = lax.axis_size(sp)
    ny = lax.axis_size("y")
    tok, width = cotangent.shape

    def flip_c(value):
        return lax.ppermute(value, "c", [(0, 1), (1, 0)])

    def flip_y(value, bit):
        return lax.ppermute(value, "y", [(i, i ^ (1 << bit)) for i in range(ny)])

    def hop(value, sign):
        pairs = []
        for y in range(ny):
            for c in range(2):
                pairs.append((2 * y + c, 2 * ((y + (sign if c == 0 else -sign)) % ny) + c))
        return lax.ppermute(value, ("y", "c"), pairs)

    rows = experts * 2 * SPAN
    ids, weights = expert_ids.T, route_weight.T
    sent, own = kernel(
        head_body,
        (shape(rows, width), shape(3, width, 128)),
        2000000000,
        ids,
        weights,
        mixer_out,
        cotangent,
        gate_weight[0],
        up_weight[0],
        down_weight[0],
        far=(2, 3, 4, 5, 6),
        far_out=(0, 1),
        scratch=(
            pltpu.VMEM((tok, width), BF),
            pltpu.VMEM((tok, width), BF),
            pltpu.VMEM((rows, width), BF),
            pltpu.VMEM((3, width, 128), BF),
            pltpu.SemaphoreType.DMA((4 + width // 128,)),
            pltpu.SemaphoreType.DMA((3 + width // 512,)),
        ),
    )
    by_y = hop(own, 1)
    by_c = flip_c(own)
    by_yc = flip_c(by_y)

    got = lax.all_to_all(sent.reshape(experts, 2 * SPAN, width), sp, 0, 0, tiled=True)
    table = kernel(table_body, shape(2 * tok, experts * 4 * SPAN), 500000000, ids, limit=12 << 10)

    act_conv, slope, vkeep, vgive = kernel(
        slope_body,
        (
            shape(tok, 128),
            shape(tok, 128, kind=F32),
            shape(ny, 2 * tok, 128, kind=F32),
            shape(ny, 2 * tok, 128),
        ),
        500000000,
        saved_normalized,
        channel_norm_gain[None, :],
        proj_weight,
        limit=16 << 10,
    )
    vgiven = flip_c(vgive)
    for bit in range(3):
        half = ny >> (bit + 1)
        vkeep, vgive = kernel(
            functools.partial(share_body, bit),
            (shape(half, 2 * tok, 128, kind=F32), shape(half, 2 * tok, 128)),
            1000000,
            vkeep,
            vgiven,
            limit=12 << 10,
        )
        vgiven = flip_y(vgive, bit)

    slots = experts * SPAN
    got = got.reshape(rows, width)
    hidden, back = kernel(
        expert_body,
        (shape(slots, 1536), shape(experts // 2, 128, 128)),
        4000000000,
        got,
        own,
        by_c,
        by_y,
        by_yc,
        far=(1, 2, 3, 4),
        limit=52 << 10,
        scratch=(
            pltpu.VMEM((slots, width), BF),
            pltpu.VMEM((slots, width), BF),
            pltpu.VMEM((width, 1024), BF),
            pltpu.VMEM((width // 128, 512, 128), BF),
            pltpu.SemaphoreType.DMA((4, 3)),
        ),
    )
    home = lax.all_to_all(
        back.reshape(experts * ny, 2 * SPAN, 128), ("z", "x", "y"), 0, 0, tiled=True
    ).reshape(-1, 128)

    packed = shape(2, 3, width, 128)
    quarter = pl.BlockSpec((2, 3, width // 4, 128), lambda j: (0, 0, j, 0))
    keep, give = pl.pallas_call(
        grads_body,
        grid=(4,),
        out_shape=(packed, packed),
        in_specs=[
            pl.BlockSpec((rows, width // 4), lambda j: (0, j)),
            pl.BlockSpec((slots, 1536), lambda j: (0, 0)),
        ],
        out_specs=[quarter, quarter],
        cost_estimate=pl.CostEstimate(flops=8000000000, bytes_accessed=7 << 20, transcendentals=0),
    )(got, hidden)
    given = flip_c(give)
    block = pl.BlockSpec((2, 1, width, 128), lambda m: (0, m, 0, 0))
    piece = pl.BlockSpec((1, width, 128), lambda m: (m, 0, 0))
    before, passing = pl.pallas_call(
        sumout_body,
        grid=(3,),
        out_shape=(shape(3, width, 128), shape(3, width, 128)),
        in_specs=[block, block],
        out_specs=[piece, piece],
        cost_estimate=pl.CostEstimate(flops=1000000, bytes_accessed=9 << 20, transcendentals=0),
    )(keep, given)
    passed = hop(passing, -1)
    grad_gate, grad_up, grad_down = kernel(
        addup_body,
        (shape(width, 128), shape(width, 128), shape(128, width)),
        1000000,
        before,
        passed,
        limit=20 << 10,
    )

    mine, other = kernel(
        combine_body,
        (shape(tok, 128, kind=F32), shape(tok, 128)),
        200000000,
        table,
        home,
        cotangent,
        far=(2,),
        limit=12 << 10,
        scratch=(pltpu.VMEM((tok, 128), BF), pltpu.SemaphoreType.DMA),
    )
    other = flip_c(other)
    mix = kernel(
        mix_body,
        shape(2 * ny, tok + 8, 128),
        1000000,
        mine,
        other,
        vkeep,
        vgiven,
        far_out=(0,),
        limit=12 << 10,
        scratch=(pltpu.VMEM((tok + 8, 128), BF), pltpu.SemaphoreType.DMA((2 * ny,))),
    )
    mix_all = lax.all_to_all(mix, ("y", "c"), 0, 0, tiled=True)

    proj = kernel(
        proj_body,
        shape(width, 128),
        300000000,
        mix_all,
        act_conv,
        far_out=(0,),
        limit=12 << 10,
        scratch=(pltpu.VMEM((width, 128), BF), pltpu.SemaphoreType.DMA((ny // 2,))),
    )
    proj = lax.all_to_all(proj.reshape(experts, -1, 128), sp, 0, 0, tiled=True)
    grad_proj = kernel(
        reduce_body, shape(width // experts, 128, kind=F32), 1000000, proj, limit=12 << 10
    )
    conv = kernel(
        norm_body,
        shape(tok, 128, kind=F32),
        500000000,
        mix_all,
        proj_weight,
        slope,
        saved_normalized,
        inverse_deviation[None, :],
        limit=16 << 10,
    )
    reach = taps.shape[0] - 1
    beyond = lax.ppermute(conv[:reach], sp, [(i + 1, i) for i in range(experts - 1)])
    extended = jnp.concatenate([conv, beyond], axis=0)
    result = jnp.zeros_like(conv)
    for j in range(reach + 1):
        result = result + taps[j][None, :] * extended[j : j + tok]
    return (result.astype(BF), grad_proj, grad_gate[None], grad_up[None], grad_down[None])


def solution(mesh):
    fine = Mesh(mesh.devices.reshape(8, 4, 8, 2), ("z", "x", "y", "c"))
    sp, tp = ("z", "x"), ("y", "c")
    return jax.shard_map(
        shards,
        mesh=fine,
        in_specs=(
            P(sp, None),
            P(sp, None),
            P(sp, None),
            P(sp, None),
            P(sp, tp),
            P(sp),
            P(tp),
            P(None, tp),
            P(tp, None),
            P(sp, None, tp),
            P(sp, None, tp),
            P(sp, tp, None),
        ),
        out_specs=(
            P(sp, tp),
            P(sp, tp),
            P(sp, None, tp),
            P(sp, None, tp),
            P(sp, tp, None),
        ),
        check_vma=False,
    )
```
